512 devices in a mesh: ep: 32 (over z, x), tp: 16 (over y, core).
Axes of the slice: x: 4, y: 8, z: 8, core: 2. Of those that a mesh axis runs over, the one named last changes fastest.
Arguments:
- mixer_rows: bfloat16 [4096, 2048], P('ep'), may hold values from -40 to 40
- mixer_gain: float32 [2048], replicated, may hold values from 0.1 to 1.9
- inner_weight: bfloat16 [2048, 1024], P(None, 'tp'), may hold values from -0.125 to 0.125
- gate_in_weight: bfloat16 [2048, 1024], P(None, 'tp'), may hold values from -0.125 to 0.125
- gate_out_weight: bfloat16 [2048, 1024], P(None, 'tp'), may hold values from -0.125 to 0.125
- conv_taps: float32 [3, 1024], P(None, 'tp'), may hold values from -3.5 to 3.5
- mixer_out_weight: bfloat16 [1024, 2048], P('tp'), may hold values from -0.1875 to 0.1875
- routed_rows: bfloat16 [8192, 2048], P('ep'), may hold values from -40 to 40
- routed_gain: float32 [2048], replicated, may hold values from 0.1 to 1.9
- route_ids: int32 [8192, 2], P('ep'), may hold values from 0 to 31, all different within a row; in each aligned block of 256 rows (0 to 255, 256 to 511, ...) at most 32 rows name the same one
- route_weights: float32 [8192, 2], P('ep'), may hold values from 0.25 to 1
- expert_gate: bfloat16 [32, 2048, 2048], P('ep', None, 'tp'), may hold values from -0.125 to 0.125
- expert_up: bfloat16 [32, 2048, 2048], P('ep', None, 'tp'), may hold values from -0.125 to 0.125
- expert_down: bfloat16 [32, 2048, 2048], P('ep', 'tp'), may hold values from -0.125 to 0.125
Outputs:
- mixer_output: bfloat16 [4096, 2048], P('ep')
- routed_output: bfloat16 [8192, 2048], P('ep')
The draws below stay inside these ranges and needn't reach their ends.
Inputs may be any that keep to these rules, and one draw needn't show every extreme that they name: `route_ids`: within each aligned block of 256 tokens, no expert is named by more than 32 choices, a bound that some block reaches; a token's 2 experts differ.
All inputs are finite; a program needn't handle non-finite values.
Results may differ from the reference program's by a relative error of at most 0.019.
Values may be sent and summed in bfloat16 or wider, within the bound.
No kernel may reach another device: no remote copies, remote signals or barrier semaphores. Data moves between devices by JAX's collectives and lax.ppermute only.
A program may use at most 64 MiB of HBM per device.

```python
import math
import jax
import jax.numpy as jnp
import numpy as np
from jax import lax

D = 2048
CONV = 1024
TAPS = 3
FF = 2048
TOPK = 2
EXPERTS = 32
TOK2 = 256
TOKENS1 = 4096
TOKENS2 = 8192
CAP = 32
N_TP = 16


def scaled_rows(key, row_total, model_width):
    keys = jax.random.split(key, 3)
    row_scale = jnp.exp(jax.random.uniform(keys[0], (row_total, 1), jnp.float32) * math.log(10.0))
    col_scale = jnp.exp(jax.random.uniform(keys[1], (1, model_width), jnp.float32) * math.log(10.0))
    base = jnp.clip(jax.random.normal(keys[2], (row_total, model_width), jnp.float32), -4.0, 4.0)
    return (base * row_scale * col_scale * 0.1).astype(jnp.bfloat16)


def draw_mixer_rows(key, part):
    return scaled_rows(jax.random.fold_in(key, 11), TOKENS1, D)


def draw_routed_rows(key, part):
    return scaled_rows(jax.random.fold_in(key, 23), TOKENS2, D)


def steps_of(stream_key, shape, pieces, least, top_value):
    loudness, own = 1.0, jax.random.fold_in(stream_key, 6)
    for dim, blocks in pieces:
        steps = jnp.exp(jax.random.uniform(jax.random.fold_in(own, dim), (blocks,), jnp.float32, least / len(pieces), top_value / len(pieces)))
        loudness = loudness * jnp.repeat(steps, shape[dim] // blocks).reshape([-1 if axis == dim else 1 for axis in range(len(shape))])
    return loudness


def assign_block(stream_key, own, number, rows, count, top, most, lean):
    order = jax.random.permutation(stream_key, count)
    crowded, usual = load_shares(count, rows * top, most, lean, True), load_shares(count, rows * top, most, lean, False)
    places = jnp.arange(count)

    def named(sizes, turn):
        used = int((sizes > 0).sum())
        fixed = max(1, used // 4)
        passed = fixed + (places - fixed + turn * (used - fixed)) % max(1, count - fixed)
        return jnp.zeros((count,), jnp.int32).at[order[jnp.where(places < fixed, places, passed)]].set(jnp.asarray(sizes, jnp.int32))

    sizes = jnp.where(number % 4 == 0, named(crowded, number // 4), named(usual, number - number // 4 - 1))
    mixed = jax.random.permutation(jax.random.fold_in(own, 3), count)
    donor, taker = mixed[0:count // 2 * 2:2], mixed[1:count // 2 * 2:2]
    room = jnp.minimum(sizes[donor] - 1, most - sizes[taker]) // 2
    room = jnp.where((donor == order[0]) | (taker == order[0]) | (sizes[taker] == 0), 0, jnp.maximum(room, 0))
    passed = jax.random.randint(jax.random.fold_in(own, 4), (count // 2,), 0, 1 << 20) % (room + 1)
    sizes = sizes.at[donor].add(-passed).at[taker].add(passed)
    members = jnp.searchsorted(jnp.cumsum(sizes), jnp.arange(rows * top), side="right").astype(jnp.int32)
    listing = members.reshape(top, rows).T
    listing = listing[jax.random.permutation(jax.random.fold_in(own, 1), rows)]
    turn = jax.random.randint(jax.random.fold_in(own, 2), (rows, 1), 0, top)
    return jnp.take_along_axis(listing, (jnp.arange(top)[None, :] + turn) % top, axis=1)


def load_shares(number_of, total, limit, skew, full):
    loads = [(1 << 20) // math.isqrt(grade ** skew) + 1 for grade in range(1, number_of + 1)]
    largest = limit if full else min(limit, max(-(-total // number_of), total * loads[0] // sum(loads)))
    least = 1 if total - largest >= number_of - 1 else 0
    given, surplus = [largest] + [least] * (number_of - 1), total - largest - least * (number_of - 1)
    while surplus > 0:
        movable = [i for i in range(1, number_of) if given[i] < largest] or [i for i in range(1, number_of) if given[i] < limit]
        mass, left = sum([loads[i] for i in movable]), surplus
        for i in movable:
            extra = min(limit - given[i], max(1, left * loads[i] // mass), surplus)
            given[i] = given[i] + extra
            surplus = surplus - extra
    return np.array(given)


def noise(key, dims, scale, bound, cuts=(), kind=jnp.bfloat16):
    loudness = steps_of(key, dims, cuts, -0.22, 0.18) if cuts else 1.0
    entries = jax.random.normal(key, dims, jnp.float32) * scale * loudness
    return jnp.minimum(jnp.maximum(entries, -bound), bound).astype(kind)


def setup_inputs(seed: int = 0) -> dict:
    arg_keys = jax.random.split(jax.random.key(seed), 15)
    mixer_rows = draw_mixer_rows(jax.random.fold_in(arg_keys[14], 71), 0)
    mixer_gain = jnp.clip(1.0 + 0.18 * jax.random.normal(arg_keys[1], (D,), jnp.float32), 0.1, 1.9)
    inner_weight = noise(arg_keys[2], (D, CONV), D ** -0.5, 0.125, ((1, 16),))
    gate_in_weight = noise(arg_keys[3], (D, CONV), D ** -0.5, 0.125, ((1, 16),))
    gate_out_weight = noise(arg_keys[4], (D, CONV), D ** -0.5, 0.125, ((1, 16),))
    conv_taps = noise(arg_keys[5], (TAPS, CONV), TAPS ** -0.5, 3.5, ((1, 16),), jnp.float32)
    mixer_out_weight = noise(arg_keys[6], (CONV, D), CONV ** -0.5, 0.1875, ((0, 16),))
    routed_rows = draw_routed_rows(jax.random.fold_in(arg_keys[14], 71), 0)
    routed_gain = jnp.clip(1.0 + 0.18 * jax.random.normal(arg_keys[8], (D,), jnp.float32), 0.1, 1.9)
    route_ids_keys = jax.random.split(jax.random.fold_in(arg_keys[9], 1), TOKENS2 // TOK2)
    route_ids_turns = jax.random.permutation(jax.random.fold_in(arg_keys[9], 3), TOKENS2 // TOK2)
    route_ids = jax.vmap(lambda own, number: assign_block(jax.random.fold_in(arg_keys[9], 2), own, number, TOK2, EXPERTS, TOPK, CAP, 2))(route_ids_keys, route_ids_turns).reshape((TOKENS2, TOPK))
    route_weights = jnp.clip(0.25 + 0.75 * jax.random.uniform(arg_keys[10], (TOKENS2, TOPK), jnp.float32) ** steps_of(arg_keys[10], (TOKENS2, TOPK), ((0, 32),), -0.2, 0.2), 0.25, 1.0)
    expert_gate = noise(arg_keys[11], (EXPERTS, D, FF), D ** -0.5, 0.125, ((0, 32), (2, 16)))
    expert_up = noise(arg_keys[12], (EXPERTS, D, FF), D ** -0.5, 0.125, ((0, 32), (2, 16)))
    expert_down = noise(arg_keys[13], (EXPERTS, FF, D), FF ** -0.5, 0.125, ((0, 32), (1, 16)))
    return dict(mixer_rows=mixer_rows, mixer_gain=mixer_gain, inner_weight=inner_weight, gate_in_weight=gate_in_weight, gate_out_weight=gate_out_weight, conv_taps=conv_taps, mixer_out_weight=mixer_out_weight, routed_rows=routed_rows, routed_gain=routed_gain, route_ids=route_ids, route_weights=route_weights, expert_gate=expert_gate, expert_up=expert_up, expert_down=expert_down)


def rms_scale(row_block, gain_row):
    values = row_block.astype(jnp.float32)
    scaled = values * lax.rsqrt(lax.optimization_barrier(jnp.mean(values * values, axis=-1, keepdims=True)) + 1e-06)
    return (scaled * gain_row).astype(jnp.bfloat16)

def rounded_again(partial_value):
    return lax.optimization_barrier(partial_value.astype(jnp.bfloat16)).astype(jnp.float32)

def reference(mixer_rows, mixer_gain, inner_weight, gate_in_weight, gate_out_weight, conv_taps, mixer_out_weight, routed_rows, routed_gain, route_ids, route_weights, expert_gate, expert_up, expert_down):
    normed = rms_scale(mixer_rows, mixer_gain)
    inner_proj = jnp.dot(normed, inner_weight, preferred_element_type=jnp.float32)
    gate_in = jnp.dot(normed, gate_in_weight, preferred_element_type=jnp.float32)
    conv_input = (gate_in * inner_proj).astype(jnp.bfloat16)
    gate_out = jnp.dot(normed, gate_out_weight, preferred_element_type=jnp.float32)
    padded = jnp.concatenate([jnp.zeros((TAPS - 1, CONV), jnp.bfloat16), conv_input], axis=0).astype(jnp.float32)
    conv_out = jnp.zeros((TOKENS1, CONV), jnp.float32)
    for tap_index in range(TAPS):
        conv_out = conv_out + conv_taps[tap_index] * padded[tap_index:tap_index + TOKENS1]
    gated_conv = (gate_out * conv_out).astype(jnp.bfloat16)
    group_width = CONV // N_TP
    running = jnp.zeros((TOKENS1, D), jnp.float32)
    for piece_index in range(N_TP):
        lower_edge = piece_index * group_width
        partial_value = jnp.dot(gated_conv[:, lower_edge:lower_edge + group_width], mixer_out_weight[lower_edge:lower_edge + group_width], preferred_element_type=jnp.float32)
        running = running + rounded_again(partial_value)
    mixer_output = running.astype(jnp.bfloat16)
    routed_normed = rms_scale(routed_rows, routed_gain)
    blocks = TOKENS2 // TOK2
    flat_ids = route_ids.reshape(blocks, TOK2 * TOPK).astype(jnp.int32)
    onehot = (flat_ids[:, :, None] == jnp.arange(EXPERTS, dtype=jnp.int32)[None, None, :]).astype(jnp.int32)
    earlier = (jnp.cumsum(onehot, axis=1) - onehot).astype(jnp.int32)
    slot_rank = lax.optimization_barrier(jnp.sum(earlier * onehot, axis=2)).astype(jnp.int32)
    block_grid = jnp.broadcast_to(jnp.arange(blocks, dtype=jnp.int32)[:, None], flat_ids.shape)
    token_index = (block_grid * TOK2 + jnp.arange(TOK2 * TOPK, dtype=jnp.int32)[None, :] // TOPK).astype(jnp.int32)
    token_table = jnp.full((EXPERTS, blocks, CAP), TOKENS2, jnp.int32).at[flat_ids, block_grid, slot_rank].set(token_index)
    padded_rows = jnp.concatenate([routed_normed, jnp.zeros((1, D), jnp.bfloat16)], axis=0)
    hidden_width = FF // N_TP

    def one_expert(operands):
        table_rows, gate_w, up_w, down_w = operands
        slot_rows = padded_rows[table_rows.reshape(-1)]
        gate_act = jnp.dot(slot_rows, gate_w, preferred_element_type=jnp.float32)
        up_act = jnp.dot(slot_rows, up_w, preferred_element_type=jnp.float32)
        hidden = (jax.nn.silu(gate_act) * up_act).astype(jnp.bfloat16)
        summed = jnp.zeros((slot_rows.shape[0], D), jnp.float32)
        for piece_index in range(N_TP):
            lower_edge = piece_index * hidden_width
            partial_value = jnp.dot(hidden[:, lower_edge:lower_edge + hidden_width], down_w[lower_edge:lower_edge + hidden_width], preferred_element_type=jnp.float32)
            summed = summed + rounded_again(partial_value)
        return summed.astype(jnp.bfloat16)
    results = lax.map(one_expert, (token_table, expert_gate, expert_up, expert_down))
    results = results.reshape(EXPERTS, blocks, CAP, D)
    picked = results[flat_ids, block_grid, slot_rank].reshape(TOKENS2, TOPK, D).astype(jnp.float32)
    picked = picked * route_weights[:, :, None]
    owner_piece = (slot_rank // (CAP // N_TP)).reshape(TOKENS2, TOPK)
    running_two = jnp.zeros((TOKENS2, D), jnp.float32)
    for piece_index in range(N_TP):
        partial_value = lax.optimization_barrier(jnp.sum(jnp.where((owner_piece == piece_index)[:, :, None], picked, jnp.float32(0.0)), axis=1))
        running_two = running_two + rounded_again(partial_value)
    routed_output = running_two.astype(jnp.bfloat16)
    return (mixer_output, routed_output)
```

```python
import functools

import jax
import jax.numpy as jnp
from jax import lax
from jax.experimental import pallas as pl
from jax.experimental.pallas import tpu as pltpu
from jax.sharding import Mesh, PartitionSpec as P

TP = ("p", "q", "c")
ALL = ("ep", "p", "q", "c")
VM = pl.BlockSpec(memory_space=pltpu.VMEM)


def rms_scale(row_block, gain_row):
    values = row_block.astype(jnp.float32)
    scaled = values * lax.rsqrt(jnp.mean(values * values, axis=-1, keepdims=True) + 1e-06)
    return (scaled * gain_row).astype(jnp.bfloat16)


def flipped(value, axis):
    return lax.ppermute(value, axis, [(0, 1), (1, 0)])


def ffn_kernel(x_ref, a0, a1, a2, a3, d0, d1, d2, d3, out_ref, hid_ref):
    x = x_ref[...]
    width = x.shape[1]
    part = a0.shape[1]
    for i, a in enumerate((a0, a1, a2, a3)):
        gate = jnp.dot(x, a[:width, :], preferred_element_type=jnp.float32)
        up = jnp.dot(x, a[width:, :], preferred_element_type=jnp.float32)
        hid_ref[:, i * part : (i + 1) * part] = (gate / (1.0 + jnp.exp(-gate)) * up).astype(jnp.bfloat16)
    cols = 512
    for n in range(0, out_ref.shape[1], cols):
        total = None
        for i, d in enumerate((d0, d1, d2, d3)):
            term = jnp.dot(
                hid_ref[:, i * part : (i + 1) * part],
                d[:, n : n + cols],
                preferred_element_type=jnp.float32,
            )
            total = term if total is None else total + term
        out_ref[:, n : n + cols] = total.astype(jnp.bfloat16)


def expert_ffn(x, gates, downs):
    hidden = sum(d.shape[0] for d in downs)
    return pl.pallas_call(
        ffn_kernel,
        out_shape=jax.ShapeDtypeStruct(x.shape, jnp.bfloat16),
        in_specs=[VM] * 9,
        out_specs=VM,
        scratch_shapes=[pltpu.VMEM((x.shape[0], hidden), jnp.bfloat16)],
        name="expert_ffn",
    )(x, *gates, *downs)


def combine_kernel(keys_ref, weights_ref, rows_ref, out_ref):
    experts, groups, capacity, width = rows_ref.shape
    tokens, picks = keys_ref.shape
    slots = experts * capacity
    column = lax.broadcasted_iota(jnp.int32, (tokens, slots), 1)
    spread = jnp.zeros((tokens, slots), jnp.float32)
    for k in range(picks):
        spread = jnp.where(column == keys_ref[:, k : k + 1], weights_ref[:, k : k + 1], spread)
    high = spread.astype(jnp.bfloat16)
    low = (spread - high.astype(jnp.float32)).astype(jnp.bfloat16)
    total = jnp.zeros((tokens, width), jnp.float32)
    for g in range(groups):
        rows = rows_ref[:, g].reshape(slots, width)
        total = total + jnp.dot(high, rows, preferred_element_type=jnp.float32)
        total = total + jnp.dot(low, rows, preferred_element_type=jnp.float32)
    out_ref[...] = total.astype(jnp.bfloat16)


def combined(keys, weights, rows):
    return pl.pallas_call(
        combine_kernel,
        out_shape=jax.ShapeDtypeStruct((keys.shape[0], rows.shape[-1]), jnp.bfloat16),
        in_specs=[VM] * 3,
        out_specs=VM,
        name="combine",
    )(keys, weights, rows)


def on_device(
    mixer_rows,
    mixer_gain,
    inner_weight,
    gate_in_weight,
    gate_out_weight,
    conv_taps,
    mixer_out_weight,
    routed_rows,
    routed_gain,
    route_ids,
    route_weights,
    expert_gate,
    expert_up,
    expert_down,
):
    experts = lax.axis_size("ep")
    groups = lax.axis_size("p")
    parts = lax.axis_size(TP)
    sharers = lax.axis_size(("q", "c"))
    quarter = lax.axis_index(("q", "c"))
    tok_count, pick_count = route_ids.shape
    width = routed_rows.shape[1]
    capacity = 2 * tok_count * pick_count // experts
    share = capacity // sharers
    piece = width // parts

    gate_up = jnp.concatenate([expert_gate[0], expert_up[0]], axis=0)
    down = expert_down[0]
    gate_up_q = flipped(gate_up, "q")
    down_q = flipped(down, "q")
    gate_up_c = flipped(gate_up, "c")
    down_c = flipped(down, "c")
    gate_up_qc = flipped(gate_up_q, "c")
    down_qc = flipped(down_q, "c")

    flat_ids = route_ids.reshape(-1)
    choices = tok_count * pick_count
    onehot = flat_ids[:, None] == jnp.arange(experts, dtype=jnp.int32)[None, :]
    before = jnp.arange(choices)[:, None] > jnp.arange(choices)[None, :]
    earlier = jnp.dot(
        before.astype(jnp.bfloat16), onehot.astype(jnp.bfloat16), preferred_element_type=jnp.float32
    )
    slot_rank = jnp.sum(jnp.where(onehot, earlier, 0.0), axis=1).astype(jnp.int32)
    keys = (flat_ids * capacity + slot_rank).reshape(tok_count, pick_count)

    routed_normed = rms_scale(routed_rows, routed_gain)
    slot_of_row = jnp.arange(experts * share, dtype=jnp.int32)
    slot_of_row = slot_of_row // share * capacity + quarter * share + slot_of_row % share
    pick = jnp.any(keys.T[:, None, :] == slot_of_row[None, :, None], axis=0)
    outgoing = jnp.dot(
        pick.astype(jnp.bfloat16), routed_normed, preferred_element_type=jnp.float32
    ).astype(jnp.bfloat16)
    slot_rows = lax.all_to_all(
        outgoing.reshape(experts, share, width), "ep", split_axis=0, concat_axis=0, tiled=True
    ).reshape(experts * share, width)

    normed = rms_scale(mixer_rows, mixer_gain)
    inner_proj = jnp.dot(normed, inner_weight, preferred_element_type=jnp.float32)
    gate_in = jnp.dot(normed, gate_in_weight, preferred_element_type=jnp.float32)
    conv_input = (gate_in * inner_proj).astype(jnp.bfloat16)
    gate_out = jnp.dot(normed, gate_out_weight, preferred_element_type=jnp.float32)
    tap_total = conv_taps.shape[0]
    length = conv_input.shape[0]
    earlier_rows = lax.ppermute(
        conv_input[length - (tap_total - 1) :], "ep", [(i, i + 1) for i in range(experts - 1)]
    )
    extended = jnp.concatenate([earlier_rows, conv_input], axis=0).astype(jnp.float32)
    conv_out = jnp.zeros(conv_input.shape, jnp.float32)
    for tap_index in range(tap_total):
        conv_out = conv_out + conv_taps[tap_index] * extended[tap_index : tap_index + length]
    gated_conv = (gate_out * conv_out).astype(jnp.bfloat16)
    mixer_terms = jnp.dot(gated_conv, mixer_out_weight, preferred_element_type=jnp.float32).astype(jnp.bfloat16)
    mixer_parts = lax.all_to_all(
        mixer_terms.reshape(length, parts, piece).transpose(1, 0, 2), TP, split_axis=0, concat_axis=0, tiled=True
    )
    mixer_piece = jnp.sum(mixer_parts.astype(jnp.float32), axis=0).astype(jnp.bfloat16)

    results = expert_ffn(
        slot_rows,
        (gate_up, gate_up_c, gate_up_q, gate_up_qc),
        (down, down_c, down_q, down_qc),
    )
    back = results.reshape(experts, share, parts, piece).transpose(0, 2, 1, 3)
    back = lax.all_to_all(
        back.reshape(experts * parts, share, piece), ALL, split_axis=0, concat_axis=0, tiled=True
    )
    routed_piece = combined(keys, route_weights, back.reshape(experts, groups, capacity, piece))

    pieces = jnp.concatenate([mixer_piece, routed_piece], axis=0)
    mine = lax.all_gather(pieces, ("p", "q"), axis=0, tiled=False)
    other = flipped(mine, "c")
    core = lax.axis_index("c")
    even = jnp.where(core == 0, mine, other)
    odd = jnp.where(core == 0, other, mine)
    whole = jnp.stack([even, odd], axis=1).reshape(parts, length + tok_count, piece)
    whole = whole.transpose(1, 0, 2).reshape(length + tok_count, width)
    return whole[:length], whole[length:]


def solution(mesh):
    experts, parts = mesh.devices.shape
    finer = Mesh(mesh.devices.reshape(experts, parts // 4, 2, 2), ALL)
    return jax.shard_map(
        on_device,
        mesh=finer,
        in_specs=(
            P("ep", None),
            P(),
            P(None, TP),
            P(None, TP),
            P(None, TP),
            P(None, TP),
            P(TP, None),
            P("ep", None),
            P(),
            P("ep", None),
            P("ep", None),
            P("ep", None, TP),
            P("ep", None, TP),
            P("ep", TP, None),
        ),
        out_specs=(P("ep", None), P("ep", None)),
        check_vma=False,
    )
```

```python
import functools

import jax
import jax.numpy as jnp
from jax import lax
from jax.experimental import pallas as pl
from jax.experimental.pallas import tpu as pltpu
from jax.sharding import Mesh, PartitionSpec as P

TP = ("p", "q", "c")
ALL = ("ep", "p", "q", "c")
VM = pl.BlockSpec(memory_space=pltpu.VMEM)


def rms_scale(row_block, gain_row):
    values = row_block.astype(jnp.float32)
    scaled = values * lax.rsqrt(jnp.mean(values * values, axis=-1, keepdims=True) + 1e-06)
    return (scaled * gain_row).astype(jnp.bfloat16)


def flipped(value, axis):
    return lax.ppermute(value, axis, [(0, 1), (1, 0)])


def route_kernel(quarter_ref, ids_ref, rows_ref, gain_ref, out_ref, keys_ref, *, capacity, share):
    tokens, picks = ids_ref.shape
    slots = out_ref.shape[0]
    lane = lax.broadcasted_iota(jnp.int32, (tokens, 128), 1)
    named = [ids_ref[:, k : k + 1] == lane for k in range(picks)]
    both = functools.reduce(jnp.logical_or, named)
    row = lax.broadcasted_iota(jnp.int32, (tokens, tokens), 0)
    col = lax.broadcasted_iota(jnp.int32, (tokens, tokens), 1)
    earlier = jnp.dot(
        jnp.where(row > col, 1.0, 0.0).astype(jnp.bfloat16),
        jnp.where(both, 1.0, 0.0).astype(jnp.bfloat16),
        preferred_element_type=jnp.float32,
    )
    slot = lax.broadcasted_iota(jnp.int32, (tokens, slots), 1)
    slot_key = slot // share * capacity + slot % share + quarter_ref[0] * share
    chosen = None
    for k in range(picks):
        rank = jnp.sum(jnp.where(named[k], earlier, 0.0), axis=1, keepdims=True).astype(jnp.int32)
        key = ids_ref[:, k : k + 1] * capacity + rank
        keys_ref[:, k : k + 1] = key
        here = key == slot_key
        chosen = here if chosen is None else jnp.logical_or(chosen, here)
    values = rows_ref[...].astype(jnp.float32)
    scaled = values * lax.rsqrt(jnp.mean(values * values, axis=-1, keepdims=True) + 1e-06)
    normed = (scaled * gain_ref[...]).astype(jnp.bfloat16)
    out_ref[...] = lax.dot_general(
        jnp.where(chosen, 1.0, 0.0).astype(jnp.bfloat16),
        normed,
        (((0,), (0,)), ((), ())),
        preferred_element_type=jnp.float32,
    ).astype(jnp.bfloat16)


def routed_slots(quarter, ids, rows, gain, experts, capacity, share):
    return pl.pallas_call(
        functools.partial(route_kernel, capacity=capacity, share=share),
        out_shape=(
            jax.ShapeDtypeStruct((experts * share, rows.shape[1]), jnp.bfloat16),
            jax.ShapeDtypeStruct(ids.shape, jnp.int32),
        ),
        in_specs=[pl.BlockSpec(memory_space=pltpu.SMEM), VM, VM, VM],
        out_specs=(VM, VM),
        name="route",
    )(quarter.reshape(1), ids, rows, gain.reshape(1, -1))


def halved(value, axis, first):
    middle = value.shape[1] // 2
    left, right = value[:, :middle], value[:, middle:]
    received = flipped(jnp.where(first, right, left), axis)
    kept = jnp.where(first, left, right)
    return (kept.astype(jnp.float32) + received.astype(jnp.float32)).astype(jnp.bfloat16)


def ffn_kernel(x_hbm, a0, a1, a2, a3, b0, b1, b2, b3, out_ref, x_ref, gu_ref, down_ref, hid_ref, sems):
    width = x_ref.shape[1]
    part = a0.shape[1]
    lead = b0.shape[0] - part
    x_copy = pltpu.make_async_copy(x_hbm, x_ref, sems.at[0])
    x_copy.start()
    copies = []
    for i, (a, b) in enumerate(((a0, b0), (a1, b1), (a2, b2), (a3, b3))):
        gate = pltpu.make_async_copy(
            a.at[pl.ds(0, width), :], gu_ref.at[i, :, pl.ds(0, part)], sems.at[3 * i + 1]
        )
        up = pltpu.make_async_copy(
            a.at[pl.ds(width, width), :], gu_ref.at[i, :, pl.ds(part, part)], sems.at[3 * i + 2]
        )
        down = pltpu.make_async_copy(
            b.at[pl.ds(lead, part), :], down_ref.at[pl.ds(i * part, part), :], sems.at[3 * i + 3]
        )
        gate.start()
        up.start()
        copies.append((gate, up, down))
    for _, _, down in copies:
        down.start()
    x_copy.wait()
    for i, (gate, up, _) in enumerate(copies):
        gate.wait()
        up.wait()
        acts = jnp.dot(x_ref[...], gu_ref[i], preferred_element_type=jnp.float32)
        g = acts[:, :part]
        hid_ref[:, i * part : (i + 1) * part] = (g / (1.0 + jnp.exp(-g)) * acts[:, part:]).astype(jnp.bfloat16)
    for _, _, down in copies:
        down.wait()
    cols = 512
    for n in range(0, width, cols):
        out_ref[:, n : n + cols] = jnp.dot(
            hid_ref[...], down_ref[:, n : n + cols], preferred_element_type=jnp.float32
        ).astype(jnp.bfloat16)


def expert_ffn(x, packs, hidden):
    rows, width = x.shape
    part = packs[0].shape[1]
    hbm = pl.BlockSpec(memory_space=pltpu.HBM)
    views = [wide_view(w, width) for w in packs]
    return pl.pallas_call(
        ffn_kernel,
        out_shape=jax.ShapeDtypeStruct(x.shape, jnp.bfloat16),
        in_specs=[hbm] * 9,
        out_specs=VM,
        scratch_shapes=[
            pltpu.VMEM((rows, width), jnp.bfloat16),
            pltpu.VMEM((4, width, 2 * part), jnp.bfloat16),
            pltpu.VMEM((hidden, width), jnp.bfloat16),
            pltpu.VMEM((rows, hidden), jnp.bfloat16),
            pltpu.SemaphoreType.DMA((13,)),
        ],
        cost_estimate=pl.CostEstimate(
            flops=6 * rows * width * hidden, bytes_accessed=8 * 2**20, transcendentals=rows * hidden
        ),
        name="expert_ffn",
    )(x, *packs, *views)


def narrow_view(value, part):
    rows, width = value.shape
    return value.reshape(rows // 8, 8, width // part, part).transpose(0, 2, 1, 3).reshape(-1, part)


def wide_view(value, width):
    _, part = value.shape
    return value.reshape(-1, width // part, 8, part).transpose(0, 2, 1, 3).reshape(-1, width)


def combine_kernel(keys_ref, weights_ref, rows_ref, out_ref):
    experts, groups, capacity, width = rows_ref.shape
    tokens, picks = keys_ref.shape
    slots = experts * capacity
    column = lax.broadcasted_iota(jnp.int32, (tokens, slots), 1)
    spread = jnp.zeros((tokens, slots), jnp.float32)
    for k in range(picks):
        spread = jnp.where(column == keys_ref[:, k : k + 1], weights_ref[:, k : k + 1], spread)
    high = spread.astype(jnp.bfloat16)
    low = (spread - high.astype(jnp.float32)).astype(jnp.bfloat16)
    total = jnp.zeros((tokens, 2 * width), jnp.float32)
    for g in range(0, groups, 2):
        rows = jnp.concatenate(
            [rows_ref[:, g].reshape(slots, width), rows_ref[:, g + 1].reshape(slots, width)], axis=1
        )
        total = total + jnp.dot(high, rows, preferred_element_type=jnp.float32)
        total = total + jnp.dot(low, rows, preferred_element_type=jnp.float32)
    out_ref[...] = (total[:, :width] + total[:, width:]).astype(jnp.bfloat16)


def combined(keys, weights, rows):
    return pl.pallas_call(
        combine_kernel,
        out_shape=jax.ShapeDtypeStruct((keys.shape[0], rows.shape[-1]), jnp.bfloat16),
        in_specs=[VM] * 3,
        out_specs=VM,
        name="combine",
    )(keys, weights, rows)


def assemble_kernel(core_ref, mine_ref, other_ref, out_ref):
    count, _, piece = mine_ref.shape
    first = core_ref[0] == 0
    for i in range(count):
        mine, other = mine_ref[i], other_ref[i]
        at = 2 * i * piece
        out_ref[:, at : at + piece] = jnp.where(first, mine, other)
        out_ref[:, at + piece : at + 2 * piece] = jnp.where(first, other, mine)


def assembled(core, mine, other):
    count, rows, piece = mine.shape
    return pl.pallas_call(
        assemble_kernel,
        out_shape=jax.ShapeDtypeStruct((rows, 2 * count * piece), jnp.bfloat16),
        in_specs=[pl.BlockSpec(memory_space=pltpu.SMEM), VM, VM],
        out_specs=VM,
        name="assemble",
    )(core.reshape(1), mine, other)


def column_kernel(parts_ref, out_ref, *, places):
    width = parts_ref.shape[2]
    for i, place in enumerate(places):
        out_ref[:, place * width : (place + 1) * width] = parts_ref[i]


def side_by_side(parts, places):
    count, rows, width = parts.shape
    return pl.pallas_call(
        functools.partial(column_kernel, places=places),
        out_shape=jax.ShapeDtypeStruct((rows, count * width), parts.dtype),
        in_specs=[VM],
        out_specs=VM,
        name="side_by_side",
    )(parts)


def on_device(
    mixer_rows,
    mixer_gain,
    inner_weight,
    gate_in_weight,
    gate_out_weight,
    conv_taps,
    mixer_out_weight,
    routed_rows,
    routed_gain,
    route_ids,
    route_weights,
    expert_gate,
    expert_up,
    expert_down,
):
    experts = lax.axis_size("ep")
    groups = lax.axis_size("p")
    parts = lax.axis_size(TP)
    sharers = lax.axis_size(("q", "c"))
    quarter = lax.axis_index(("q", "c"))
    tok_count, pick_count = route_ids.shape
    width = routed_rows.shape[1]
    capacity = 2 * tok_count * pick_count // experts
    share = capacity // sharers
    piece = width // parts
    hidden_part = expert_gate.shape[2]

    pack = jnp.concatenate([expert_gate[0], expert_up[0], narrow_view(expert_down[0], hidden_part)], axis=0)
    pack_q = flipped(pack, "q")
    pack_c = flipped(pack, "c")
    pack_qc = flipped(pack_q, "c")

    outgoing, keys = routed_slots(quarter, route_ids, routed_rows, routed_gain, experts, capacity, share)
    slot_rows = lax.all_to_all(
        outgoing.reshape(experts, share, width), "ep", split_axis=0, concat_axis=0, tiled=True
    ).reshape(experts * share, width)

    normed = rms_scale(mixer_rows, mixer_gain)
    inner_proj = jnp.dot(normed, inner_weight, preferred_element_type=jnp.float32)
    gate_in = jnp.dot(normed, gate_in_weight, preferred_element_type=jnp.float32)
    conv_input = (gate_in * inner_proj).astype(jnp.bfloat16)
    gate_out = jnp.dot(normed, gate_out_weight, preferred_element_type=jnp.float32)
    tap_total = conv_taps.shape[0]
    length = conv_input.shape[0]
    earlier_rows = lax.ppermute(conv_input[length - (tap_total - 1) :], "ep", [(i, i + 1) for i in range(experts - 1)])
    extended = jnp.concatenate([earlier_rows, conv_input], axis=0).astype(jnp.float32)
    conv_out = jnp.zeros(conv_input.shape, jnp.float32)
    for tap_index in range(tap_total):
        conv_out = conv_out + conv_taps[tap_index] * extended[tap_index : tap_index + length]
    gated_conv = (gate_out * conv_out).astype(jnp.bfloat16)
    mixer_terms = jnp.dot(gated_conv, mixer_out_weight, preferred_element_type=jnp.float32).astype(jnp.bfloat16)
    core, side = lax.axis_index("c") == 0, lax.axis_index("q") == 0
    mixer_half = halved(mixer_terms, "c", core)
    mixer_quarter = halved(mixer_half, "q", side)

    results = expert_ffn(slot_rows, (pack, pack_c, pack_q, pack_qc), sharers * hidden_part)
    back = results.reshape(experts, share, parts, piece).transpose(0, 2, 1, 3)
    back = lax.all_to_all(
        back.reshape(experts * parts, share, piece), ALL, split_axis=0, concat_axis=0, tiled=True
    )
    mixer_parts = lax.all_gather(mixer_quarter, "p", axis=0, tiled=False)
    mixer_quarter = jnp.sum(mixer_parts.astype(jnp.float32), axis=0).astype(jnp.bfloat16)
    mixer_whole = lax.all_gather(mixer_quarter, ("q", "c"), axis=0, tiled=False)
    mixer_whole = side_by_side(mixer_whole, (0, 2, 1, 3))
    routed_piece = combined(keys, route_weights, back.reshape(experts, groups, capacity, piece))

    mine = lax.all_gather(routed_piece, ("p", "q"), axis=0, tiled=False)
    other = flipped(mine, "c")
    return mixer_whole, assembled(lax.axis_index("c"), mine, other)


def solution(mesh):
    experts, parts = mesh.devices.shape
    finer = Mesh(mesh.devices.reshape(experts, parts // 4, 2, 2), ALL)
    return jax.shard_map(
        on_device,
        mesh=finer,
        in_specs=(
            P("ep", None),
            P(),
            P(None, TP),
            P(None, TP),
            P(None, TP),
            P(None, TP),
            P(TP, None),
            P("ep", None),
            P(),
            P("ep", None),
            P("ep", None),
            P("ep", None, TP),
            P("ep", None, TP),
            P("ep", TP, None),
        ),
        out_specs=(P("ep", None), P("ep", None)),
        check_vma=False,
    )
```

```python
import functools

import jax
import jax.numpy as jnp
from jax import lax
from jax.experimental import pallas as pl
from jax.experimental.pallas import tpu as pltpu
from jax.sharding import Mesh, PartitionSpec as P

TP = ("p", "q", "c")
ALL = ("ep", "p", "q", "c")
VM = pl.BlockSpec(memory_space=pltpu.VMEM)
HBM = pl.BlockSpec(memory_space=pltpu.HBM)


def flipped(value, axis):
    return lax.ppermute(value, axis, [(0, 1), (1, 0)])


def route_kernel(
    quarter_ref,
    ids_ref,
    weights_ref,
    rows_ref,
    gain_ref,
    gate_hbm,
    up_hbm,
    down_hbm,
    out_ref,
    picks_ref,
    pack_hbm,
    sems,
    *,
    experts,
    capacity,
    share,
):
    copies, at = [], 0
    for i, source in enumerate((gate_hbm, up_hbm, down_hbm)):
        size = source.shape[0]
        copies.append(pltpu.make_async_copy(source, pack_hbm.at[pl.ds(at, size), :], sems.at[i]))
        copies[-1].start()
        at += size
    picks, tokens = ids_ref.shape
    slots = out_ref.shape[0]
    expert = lax.broadcasted_iota(jnp.int32, (experts, tokens), 0)
    named = [ids_ref[k : k + 1, :] == expert for k in range(picks)]
    both = functools.reduce(jnp.logical_or, named)
    row = lax.broadcasted_iota(jnp.int32, (tokens, tokens), 0)
    col = lax.broadcasted_iota(jnp.int32, (tokens, tokens), 1)
    earlier = jnp.dot(
        jnp.where(both, 1.0, 0.0).astype(jnp.bfloat16),
        jnp.where(row < col, 1.0, 0.0).astype(jnp.bfloat16),
        preferred_element_type=jnp.float32,
    )
    slot = lax.broadcasted_iota(jnp.int32, (slots, tokens), 0)
    slot_key = slot // share * capacity + slot % share + quarter_ref[0] * share
    chosen, lines = None, []
    for k in range(picks):
        rank = jnp.sum(jnp.where(named[k], earlier, 0.0), axis=0, keepdims=True).astype(jnp.int32)
        key = ids_ref[k : k + 1, :] * capacity + rank
        lines.append(key.astype(jnp.float32))
        here = slot_key == key
        chosen = here if chosen is None else jnp.logical_or(chosen, here)
    lines += [weights_ref[k : k + 1, :] for k in range(picks)]
    line = lax.broadcasted_iota(jnp.int32, (128, tokens), 0)
    table = jnp.zeros((128, tokens), jnp.float32)
    for i, value in enumerate(lines):
        table = jnp.where(line == i, value, table)
    picks_ref[...] = table.T
    values = rows_ref[...].astype(jnp.float32)
    scaled = values * lax.rsqrt(jnp.mean(values * values, axis=-1, keepdims=True) + 1e-06)
    normed = (scaled * gain_ref[...]).astype(jnp.bfloat16)
    out_ref[...] = jnp.dot(
        jnp.where(chosen, 1.0, 0.0).astype(jnp.bfloat16), normed, preferred_element_type=jnp.float32
    ).astype(jnp.bfloat16)
    for copy in copies:
        copy.wait()


def routed_slots(quarter, ids, weights, rows, gain, gate, up, down, experts, capacity, share):
    tokens, width = rows.shape
    packed = gate.shape[0] + up.shape[0] + down.shape[0]
    return pl.pallas_call(
        functools.partial(route_kernel, experts=experts, capacity=capacity, share=share),
        out_shape=(
            jax.ShapeDtypeStruct((experts * share, width), jnp.bfloat16),
            jax.ShapeDtypeStruct((tokens, 128), jnp.float32),
            jax.ShapeDtypeStruct((packed, gate.shape[1]), jnp.bfloat16),
        ),
        in_specs=[pl.BlockSpec(memory_space=pltpu.SMEM), VM, VM, VM, VM, HBM, HBM, HBM],
        out_specs=(VM, VM, HBM),
        scratch_shapes=[pltpu.SemaphoreType.DMA((3,))],
        name="route",
    )(quarter.reshape(1), ids.T, weights.T, rows, gain.reshape(1, -1), gate, up, down)


def mixer_kernel(
    core_ref, before_ref, rows_ref, gain_ref, inner_ref, gate_in_ref, gate_out_ref, taps_ref, out_w_ref, keep_ref, send_ref, ext_ref
):
    def normed(ref):
        values = ref[...].astype(jnp.float32)
        scaled = values * lax.rsqrt(jnp.mean(values * values, axis=-1, keepdims=True) + 1e-06)
        return (scaled * gain_ref[...]).astype(jnp.bfloat16)

    def projected(x, ref):
        return lax.dot_general(x, ref[...], (((1,), (1,)), ((), ())), preferred_element_type=jnp.float32)

    def conv_input(x):
        return (projected(x, gate_in_ref) * projected(x, inner_ref)).astype(jnp.bfloat16).astype(jnp.float32)

    lead, length = before_ref.shape[0], rows_ref.shape[0]
    x = normed(rows_ref)
    ext_ref[:lead, :] = conv_input(normed(before_ref))
    ext_ref[lead:, :] = conv_input(x)
    taps = taps_ref.shape[0]
    conv_out = None
    for j in range(taps):
        at = lead - (taps - 1) + j
        term = taps_ref[j : j + 1, :] * ext_ref[at : at + length, :]
        conv_out = term if conv_out is None else conv_out + term
    gated = (projected(x, gate_out_ref) * conv_out).astype(jnp.bfloat16)
    middle = out_w_ref.shape[1] // 2
    left = jnp.dot(gated, out_w_ref[:, :middle], preferred_element_type=jnp.float32).astype(jnp.bfloat16)
    right = jnp.dot(gated, out_w_ref[:, middle:], preferred_element_type=jnp.float32).astype(jnp.bfloat16)
    first = core_ref[0] == 0
    keep_ref[...] = jnp.where(first, left, right)
    send_ref[...] = jnp.where(first, right, left)


def mixer_terms(core, before, rows, gain, inner, gate_in, gate_out, taps, out_weight):
    length, width = rows.shape
    half = jax.ShapeDtypeStruct((length, width // 2), jnp.bfloat16)
    return pl.pallas_call(
        mixer_kernel,
        out_shape=(half, half),
        in_specs=[pl.BlockSpec(memory_space=pltpu.SMEM)] + [VM] * 8,
        out_specs=(VM, VM),
        scratch_shapes=[pltpu.VMEM((before.shape[0] + length, taps.shape[1]), jnp.float32)],
        name="mixer",
    )(core.reshape(1), before, rows, gain.reshape(1, -1), inner.T, gate_in.T, gate_out.T, taps, out_weight)


def summed(kept, sent, axis, pairs):
    received = lax.ppermute(sent, axis, pairs)
    return (kept.astype(jnp.float32) + received.astype(jnp.float32)).astype(jnp.bfloat16)


def halves(value, first):
    middle = value.shape[1] // 2
    left, right = value[:, :middle], value[:, middle:]
    return jnp.where(first, left, right), jnp.where(first, right, left)


def ffn_kernel(x_hbm, a0, a1, a2, a3, b0, b1, b2, b3, out_ref, x_ref, gu_ref, down_ref, hid_ref, sems):
    width = x_ref.shape[1]
    part = a0.shape[1]
    lead = b0.shape[0] - part
    x_copy = pltpu.make_async_copy(x_hbm, x_ref, sems.at[0])
    x_copy.start()
    copies = []
    for i, (a, b) in enumerate(((a0, b0), (a1, b1), (a2, b2), (a3, b3))):
        gate = pltpu.make_async_copy(
            a.at[pl.ds(0, width), :], gu_ref.at[i, :, pl.ds(0, part)], sems.at[3 * i + 1]
        )
        up = pltpu.make_async_copy(
            a.at[pl.ds(width, width), :], gu_ref.at[i, :, pl.ds(part, part)], sems.at[3 * i + 2]
        )
        down = pltpu.make_async_copy(
            b.at[pl.ds(lead, part), :], down_ref.at[pl.ds(i * part, part), :], sems.at[3 * i + 3]
        )
        gate.start()
        up.start()
        copies.append((gate, up, down))
    for _, _, down in copies:
        down.start()
    x_copy.wait()
    for i, (gate, up, _) in enumerate(copies):
        gate.wait()
        up.wait()
        acts = jnp.dot(x_ref[...], gu_ref[i], preferred_element_type=jnp.float32)
        g = acts[:, :part]
        hid_ref[:, i * part : (i + 1) * part] = (g / (1.0 + jnp.exp(-g)) * acts[:, part:]).astype(jnp.bfloat16)
    for _, _, down in copies:
        down.wait()
    cols = 512
    for n in range(0, width, cols):
        out_ref[:, n : n + cols] = jnp.dot(
            hid_ref[...], down_ref[:, n : n + cols], preferred_element_type=jnp.float32
        ).astype(jnp.bfloat16)


def expert_ffn(x, packs, hidden):
    rows, width = x.shape
    part = packs[0].shape[1]
    views = [wide_view(w, width) for w in packs]
    return pl.pallas_call(
        ffn_kernel,
        out_shape=jax.ShapeDtypeStruct(x.shape, jnp.bfloat16),
        in_specs=[HBM] * 9,
        out_specs=VM,
        scratch_shapes=[
            pltpu.VMEM((rows, width), jnp.bfloat16),
            pltpu.VMEM((4, width, 2 * part), jnp.bfloat16),
            pltpu.VMEM((hidden, width), jnp.bfloat16),
            pltpu.VMEM((rows, hidden), jnp.bfloat16),
            pltpu.SemaphoreType.DMA((13,)),
        ],
        cost_estimate=pl.CostEstimate(
            flops=6 * rows * width * hidden, bytes_accessed=8 * 2**20, transcendentals=rows * hidden
        ),
        name="expert_ffn",
    )(x, *packs, *views)


def narrow_view(value, part):
    rows, width = value.shape
    return value.reshape(rows // 8, 8, width // part, part).transpose(0, 2, 1, 3).reshape(-1, part)


def wide_view(value, width):
    _, part = value.shape
    return value.reshape(-1, width // part, 8, part).transpose(0, 2, 1, 3).reshape(-1, width)


def combine_kernel(picks_ref, rows_ref, out_ref, *, picks):
    experts, groups, capacity, width = rows_ref.shape
    tokens = picks_ref.shape[0]
    slots = experts * capacity
    column = lax.broadcasted_iota(jnp.int32, (tokens, slots), 1)
    spread = jnp.zeros((tokens, slots), jnp.float32)
    for k in range(picks):
        key = picks_ref[:, k : k + 1].astype(jnp.int32)
        spread = jnp.where(column == key, picks_ref[:, picks + k : picks + k + 1], spread)
    high = spread.astype(jnp.bfloat16)
    low = (spread - high.astype(jnp.float32)).astype(jnp.bfloat16)
    total = jnp.zeros((tokens, 2 * width), jnp.float32)
    for g in range(0, groups, 2):
        rows = jnp.concatenate(
            [rows_ref[:, g].reshape(slots, width), rows_ref[:, g + 1].reshape(slots, width)], axis=1
        )
        total = total + jnp.dot(high, rows, preferred_element_type=jnp.float32)
        total = total + jnp.dot(low, rows, preferred_element_type=jnp.float32)
    out_ref[...] = (total[:, :width] + total[:, width:]).astype(jnp.bfloat16)


def combined(table, rows, picks):
    return pl.pallas_call(
        functools.partial(combine_kernel, picks=picks),
        out_shape=jax.ShapeDtypeStruct((table.shape[0], rows.shape[-1]), jnp.bfloat16),
        in_specs=[VM] * 2,
        out_specs=VM,
        name="combine",
    )(table, rows)


def assemble_kernel(core_ref, mine_ref, other_ref, mixer_ref, routed_ref):
    count, _, piece = mine_ref.shape
    length = mixer_ref.shape[0]
    first = core_ref[0] == 0
    for i in range(count):
        mine, other = mine_ref[i], other_ref[i]
        lower = jnp.where(first, mine, other)
        upper = jnp.where(first, other, mine)
        at = 2 * i * piece
        routed_ref[:, at : at + piece] = lower[length:]
        routed_ref[:, at + piece : at + 2 * piece] = upper[length:]
        at = (i % 2 * (count // 2) + i // 2) * piece
        mixer_ref[:, at : at + piece] = lower[:length]
        at += count * piece
        mixer_ref[:, at : at + piece] = upper[:length]


def assembled(core, mine, other, length):
    count, rows, piece = mine.shape
    return pl.pallas_call(
        assemble_kernel,
        out_shape=(
            jax.ShapeDtypeStruct((length, 2 * count * piece), jnp.bfloat16),
            jax.ShapeDtypeStruct((rows - length, 2 * count * piece), jnp.bfloat16),
        ),
        in_specs=[pl.BlockSpec(memory_space=pltpu.SMEM), VM, VM],
        out_specs=(VM, VM),
        name="assemble",
    )(core.reshape(1), mine, other)


def on_device(
    mixer_rows,
    mixer_gain,
    inner_weight,
    gate_in_weight,
    gate_out_weight,
    conv_taps,
    mixer_out_weight,
    routed_rows,
    routed_gain,
    route_ids,
    route_weights,
    expert_gate,
    expert_up,
    expert_down,
):
    experts = lax.axis_size("ep")
    groups = lax.axis_size("p")
    parts = lax.axis_size(TP)
    sharers = lax.axis_size(("q", "c"))
    quarter = lax.axis_index(("q", "c"))
    tok_count, pick_count = route_ids.shape
    width = routed_rows.shape[1]
    capacity = 2 * tok_count * pick_count // experts
    share = capacity // sharers
    piece = width // parts
    hidden_part = expert_gate.shape[2]

    core, side = lax.axis_index("c"), lax.axis_index("q")
    column = lax.axis_index("p")
    length = mixer_rows.shape[0]

    lead = 8
    before = lax.ppermute(mixer_rows[length - lead :], "ep", [(i, i + 1) for i in range(experts - 1)])

    outgoing, table, pack = routed_slots(
        quarter,
        route_ids,
        route_weights,
        routed_rows,
        routed_gain,
        expert_gate[0],
        expert_up[0],
        narrow_view(expert_down[0], hidden_part),
        experts,
        capacity,
        share,
    )
    pack_q = flipped(pack, "q")
    slot_rows = lax.all_to_all(
        outgoing.reshape(experts, share, width), "ep", split_axis=0, concat_axis=0, tiled=True
    ).reshape(experts * share, width)
    pack_c = flipped(pack, "c")
    pack_qc = flipped(pack_q, "c")

    keep, send = mixer_terms(
        core, before, mixer_rows, mixer_gain, inner_weight, gate_in_weight, gate_out_weight, conv_taps, mixer_out_weight
    )
    swap = [(0, 1), (1, 0)]
    mixer_part = summed(keep, send, "c", swap)
    mixer_part = summed(*halves(mixer_part, side == 0), "q", swap)
    mixer_part = summed(*halves(mixer_part, column < 2), "p", [(i, i ^ 2) for i in range(groups)])
    mixer_part = summed(*halves(mixer_part, column % 2 == 0), "p", [(i, i ^ 1) for i in range(groups)])

    results = expert_ffn(slot_rows, (pack, pack_c, pack_q, pack_qc), sharers * hidden_part)
    back = results.reshape(experts, share, parts, piece).transpose(0, 2, 1, 3)
    back = lax.all_to_all(
        back.reshape(experts * parts, share, piece), ALL, split_axis=0, concat_axis=0, tiled=True
    )
    routed_part = combined(table, back.reshape(experts, groups, capacity, piece), pick_count)

    pieces = jnp.concatenate([mixer_part, routed_part], axis=0)
    mine = lax.all_gather(pieces, ("p", "q"), axis=0, tiled=False)
    other = flipped(mine, "c")
    return assembled(core, mine, other, length)


def solution(mesh):
    experts, parts = mesh.devices.shape
    finer = Mesh(mesh.devices.reshape(experts, parts // 4, 2, 2), ALL)
    return jax.shard_map(
        on_device,
        mesh=finer,
        in_specs=(
            P("ep", None),
            P(),
            P(None, TP),
            P(None, TP),
            P(None, TP),
            P(None, TP),
            P(TP, None),
            P("ep", None),
            P(),
            P("ep", None),
            P("ep", None),
            P("ep", None, TP),
            P("ep", None, TP),
            P("ep", TP, None),
        ),
        out_specs=(P("ep", None), P("ep", None)),
        check_vma=False,
    )
```

```python
import functools

import jax
import jax.numpy as jnp
from jax import lax
from jax.experimental import pallas as pl
from jax.experimental.pallas import tpu as pltpu
from jax.sharding import Mesh, PartitionSpec as P

TP = ("p", "q", "c")
ALL = ("ep", "p", "q", "c")
VM = pl.BlockSpec(memory_space=pltpu.VMEM)
HBM = pl.BlockSpec(memory_space=pltpu.HBM)


def flipped(value, axis):
    return lax.ppermute(value, axis, [(0, 1), (1, 0)])


def route_kernel(
    quarter_ref,
    ids_ref,
    weights_ref,
    rows_ref,
    gain_ref,
    out_ref,
    picks_ref,
    *,
    experts,
    capacity,
    share,
):
    picks, tokens = ids_ref.shape
    slots = out_ref.shape[0]
    expert = lax.broadcasted_iota(jnp.int32, (experts, tokens), 0)
    named = [ids_ref[k : k + 1, :] == expert for k in range(picks)]
    both = functools.reduce(jnp.logical_or, named)
    row = lax.broadcasted_iota(jnp.int32, (tokens, tokens), 0)
    col = lax.broadcasted_iota(jnp.int32, (tokens, tokens), 1)
    earlier = jnp.dot(
        jnp.where(both, 1.0, 0.0).astype(jnp.bfloat16),
        jnp.where(row < col, 1.0, 0.0).astype(jnp.bfloat16),
        preferred_element_type=jnp.float32,
    )
    slot = lax.broadcasted_iota(jnp.int32, (slots, tokens), 0)
    slot_key = slot // share * capacity + slot % share + quarter_ref[0] * share
    chosen, lines = None, []
    for k in range(picks):
        rank = jnp.sum(jnp.where(named[k], earlier, 0.0), axis=0, keepdims=True).astype(jnp.int32)
        key = ids_ref[k : k + 1, :] * capacity + rank
        lines.append(key.astype(jnp.float32))
        here = slot_key == key
        chosen = here if chosen is None else jnp.logical_or(chosen, here)
    lines += [weights_ref[k : k + 1, :] for k in range(picks)]
    line = lax.broadcasted_iota(jnp.int32, (128, tokens), 0)
    table = jnp.zeros((128, tokens), jnp.float32)
    for i, value in enumerate(lines):
        table = jnp.where(line == i, value, table)
    picks_ref[...] = table.T
    values = rows_ref[...].astype(jnp.float32)
    scaled = values * lax.rsqrt(jnp.mean(values * values, axis=-1, keepdims=True) + 1e-06)
    normed = (scaled * gain_ref[...]).astype(jnp.bfloat16)
    out_ref[...] = jnp.dot(
        jnp.where(chosen, 1.0, 0.0).astype(jnp.bfloat16), normed, preferred_element_type=jnp.float32
    ).astype(jnp.bfloat16)


def routed_slots(quarter, ids, weights, rows, gain, experts, capacity, share):
    tokens, width = rows.shape
    return pl.pallas_call(
        functools.partial(route_kernel, experts=experts, capacity=capacity, share=share),
        out_shape=(
            jax.ShapeDtypeStruct((experts * share, width), jnp.bfloat16),
            jax.ShapeDtypeStruct((tokens, 128), jnp.float32),
        ),
        in_specs=[pl.BlockSpec(memory_space=pltpu.SMEM), VM, VM, VM, VM],
        out_specs=(VM, VM),
        name="route",
    )(quarter.reshape(1), ids.T, weights.T, rows, gain.reshape(1, -1))


def mixer_kernel(
    core_ref, before_ref, rows_ref, gain_ref, inner_ref, gate_in_ref, gate_out_ref, taps_ref, out_w_ref, keep_ref, send_ref, ext_ref
):
    def normed(ref):
        values = ref[...].astype(jnp.float32)
        scaled = values * lax.rsqrt(jnp.mean(values * values, axis=-1, keepdims=True) + 1e-06)
        return (scaled * gain_ref[...]).astype(jnp.bfloat16)

    def projected(x, ref):
        return lax.dot_general(x, ref[...], (((1,), (1,)), ((), ())), preferred_element_type=jnp.float32)

    def conv_input(x):
        return (projected(x, gate_in_ref) * projected(x, inner_ref)).astype(jnp.bfloat16).astype(jnp.float32)

    lead, length = before_ref.shape[0], rows_ref.shape[0]
    x = normed(rows_ref)
    ext_ref[:lead, :] = conv_input(normed(before_ref))
    ext_ref[lead:, :] = conv_input(x)
    taps = taps_ref.shape[0]
    conv_out = None
    for j in range(taps):
        at = lead - (taps - 1) + j
        term = taps_ref[j : j + 1, :] * ext_ref[at : at + length, :]
        conv_out = term if conv_out is None else conv_out + term
    gated = (projected(x, gate_out_ref) * conv_out).astype(jnp.bfloat16)
    middle = out_w_ref.shape[1] // 2
    left = jnp.dot(gated, out_w_ref[:, :middle], preferred_element_type=jnp.float32).astype(jnp.bfloat16)
    right = jnp.dot(gated, out_w_ref[:, middle:], preferred_element_type=jnp.float32).astype(jnp.bfloat16)
    first = core_ref[0] == 0
    keep_ref[...] = jnp.where(first, left, right)
    send_ref[...] = jnp.where(first, right, left)


def mixer_terms(core, before, rows, gain, inner, gate_in, gate_out, taps, out_weight):
    length, width = rows.shape
    half = jax.ShapeDtypeStruct((length, width // 2), jnp.bfloat16)
    return pl.pallas_call(
        mixer_kernel,
        out_shape=(half, half),
        in_specs=[pl.BlockSpec(memory_space=pltpu.SMEM)] + [VM] * 8,
        out_specs=(VM, VM),
        scratch_shapes=[pltpu.VMEM((before.shape[0] + length, taps.shape[1]), jnp.float32)],
        name="mixer",
    )(core.reshape(1), before, rows, gain.reshape(1, -1), inner.T, gate_in.T, gate_out.T, taps, out_weight)


def summed(kept, sent, axis, pairs):
    received = lax.ppermute(sent, axis, pairs)
    return (kept.astype(jnp.float32) + received.astype(jnp.float32)).astype(jnp.bfloat16)


def halves(value, first):
    middle = value.shape[1] // 2
    left, right = value[:, :middle], value[:, middle:]
    return jnp.where(first, left, right), jnp.where(first, right, left)


def ffn_kernel(x_hbm, a0, a1, a2, a3, b0, b1, b2, b3, out_ref, x_ref, gu_ref, down_ref, hid_ref, sems):
    width = x_ref.shape[1]
    part = a0.shape[1]
    lead = b0.shape[0] - part
    x_copy = pltpu.make_async_copy(x_hbm, x_ref, sems.at[0])
    x_copy.start()
    copies = []
    for i, (a, b) in enumerate(((a0, b0), (a1, b1), (a2, b2), (a3, b3))):
        gate = pltpu.make_async_copy(
            a.at[pl.ds(0, width), :], gu_ref.at[i, :, pl.ds(0, part)], sems.at[3 * i + 1]
        )
        up = pltpu.make_async_copy(
            a.at[pl.ds(width, width), :], gu_ref.at[i, :, pl.ds(part, part)], sems.at[3 * i + 2]
        )
        down = pltpu.make_async_copy(
            b.at[pl.ds(lead, part), :], down_ref.at[pl.ds(i * part, part), :], sems.at[3 * i + 3]
        )
        gate.start()
        up.start()
        copies.append((gate, up, down))
    for _, _, down in copies:
        down.start()
    x_copy.wait()
    for i, (gate, up, _) in enumerate(copies):
        gate.wait()
        up.wait()
        acts = jnp.dot(x_ref[...], gu_ref[i], preferred_element_type=jnp.float32)
        g = acts[:, :part]
        hid_ref[:, i * part : (i + 1) * part] = (g / (1.0 + jnp.exp(-g)) * acts[:, part:]).astype(jnp.bfloat16)
    for _, _, down in copies:
        down.wait()
    cols = 512
    for n in range(0, width, cols):
        out_ref[:, n : n + cols] = jnp.dot(
            hid_ref[...], down_ref[:, n : n + cols], preferred_element_type=jnp.float32
        ).astype(jnp.bfloat16)


def expert_ffn(x, packs, hidden):
    rows, width = x.shape
    part = packs[0].shape[1]
    views = [wide_view(w, width) for w in packs]
    return pl.pallas_call(
        ffn_kernel,
        out_shape=jax.ShapeDtypeStruct(x.shape, jnp.bfloat16),
        in_specs=[HBM] * 9,
        out_specs=VM,
        scratch_shapes=[
            pltpu.VMEM((rows, width), jnp.bfloat16),
            pltpu.VMEM((4, width, 2 * part), jnp.bfloat16),
            pltpu.VMEM((hidden, width), jnp.bfloat16),
            pltpu.VMEM((rows, hidden), jnp.bfloat16),
            pltpu.SemaphoreType.DMA((13,)),
        ],
        cost_estimate=pl.CostEstimate(
            flops=6 * rows * width * hidden, bytes_accessed=8 * 2**20, transcendentals=rows * hidden
        ),
        name="expert_ffn",
    )(x, *packs, *views)


def narrow_view(value, part):
    rows, width = value.shape
    return value.reshape(rows // 8, 8, width // part, part).transpose(0, 2, 1, 3).reshape(-1, part)


def wide_view(value, width):
    _, part = value.shape
    return value.reshape(-1, width // part, 8, part).transpose(0, 2, 1, 3).reshape(-1, width)


def combine_kernel(picks_ref, rows_ref, mixer_ref, out_ref, *, picks):
    experts, groups, capacity, width = rows_ref.shape
    tokens = picks_ref.shape[0]
    slots = experts * capacity
    column = lax.broadcasted_iota(jnp.int32, (tokens, slots), 1)
    spread = jnp.zeros((tokens, slots), jnp.float32)
    for k in range(picks):
        key = picks_ref[:, k : k + 1].astype(jnp.int32)
        spread = jnp.where(column == key, picks_ref[:, picks + k : picks + k + 1], spread)
    high = spread.astype(jnp.bfloat16)
    low = (spread - high.astype(jnp.float32)).astype(jnp.bfloat16)
    total = jnp.zeros((tokens, 2 * width), jnp.float32)
    for g in range(0, groups, 2):
        rows = jnp.concatenate(
            [rows_ref[:, g].reshape(slots, width), rows_ref[:, g + 1].reshape(slots, width)], axis=1
        )
        total = total + jnp.dot(high, rows, preferred_element_type=jnp.float32)
        total = total + jnp.dot(low, rows, preferred_element_type=jnp.float32)
    length = mixer_ref.shape[0]
    out_ref[:length, :] = mixer_ref[...]
    out_ref[length:, :] = (total[:, :width] + total[:, width:]).astype(jnp.bfloat16)


def combined(table, rows, mixer_part, picks):
    return pl.pallas_call(
        functools.partial(combine_kernel, picks=picks),
        out_shape=jax.ShapeDtypeStruct((mixer_part.shape[0] + table.shape[0], rows.shape[-1]), jnp.bfloat16),
        in_specs=[VM] * 3,
        out_specs=VM,
        name="combine",
    )(table, rows, mixer_part)


def assemble_kernel(core_ref, mine_ref, other_ref, mixer_ref, routed_ref):
    count, _, piece = mine_ref.shape
    length = mixer_ref.shape[0]
    first = core_ref[0] == 0
    for i in range(count):
        mine, other = mine_ref[i], other_ref[i]
        lower = jnp.where(first, mine, other)
        upper = jnp.where(first, other, mine)
        at = 2 * i * piece
        routed_ref[:, at : at + piece] = lower[length:]
        routed_ref[:, at + piece : at + 2 * piece] = upper[length:]
        at = (i % 2 * (count // 2) + i // 2) * piece
        mixer_ref[:, at : at + piece] = lower[:length]
        at += count * piece
        mixer_ref[:, at : at + piece] = upper[:length]


def assembled(core, mine, other, length):
    count, rows, piece = mine.shape
    return pl.pallas_call(
        assemble_kernel,
        out_shape=(
            jax.ShapeDtypeStruct((length, 2 * count * piece), jnp.bfloat16),
            jax.ShapeDtypeStruct((rows - length, 2 * count * piece), jnp.bfloat16),
        ),
        in_specs=[pl.BlockSpec(memory_space=pltpu.SMEM), VM, VM],
        out_specs=(VM, VM),
        name="assemble",
    )(core.reshape(1), mine, other)


def on_device(
    mixer_rows,
    mixer_gain,
    inner_weight,
    gate_in_weight,
    gate_out_weight,
    conv_taps,
    mixer_out_weight,
    routed_rows,
    routed_gain,
    route_ids,
    route_weights,
    expert_gate,
    expert_up,
    expert_down,
):
    experts = lax.axis_size("ep")
    groups = lax.axis_size("p")
    parts = lax.axis_size(TP)
    sharers = lax.axis_size(("q", "c"))
    quarter = lax.axis_index(("q", "c"))
    tok_count, pick_count = route_ids.shape
    width = routed_rows.shape[1]
    capacity = 2 * tok_count * pick_count // experts
    share = capacity // sharers
    piece = width // parts
    hidden_part = expert_gate.shape[2]

    core, side = lax.axis_index("c"), lax.axis_index("q")
    column = lax.axis_index("p")
    length = mixer_rows.shape[0]

    pack = jnp.concatenate([expert_gate[0], expert_up[0], narrow_view(expert_down[0], hidden_part)], axis=0)
    pack_q = flipped(pack, "q")

    lead = 8
    before = lax.ppermute(mixer_rows[length - lead :], "ep", [(i, i + 1) for i in range(experts - 1)])

    outgoing, table = routed_slots(
        quarter, route_ids, route_weights, routed_rows, routed_gain, experts, capacity, share
    )
    slot_rows = lax.all_to_all(
        outgoing.reshape(experts, share, width), "ep", split_axis=0, concat_axis=0, tiled=True
    ).reshape(experts * share, width)
    pack_c = flipped(pack, "c")
    pack_qc = flipped(pack_q, "c")

    keep, send = mixer_terms(
        core, before, mixer_rows, mixer_gain, inner_weight, gate_in_weight, gate_out_weight, conv_taps, mixer_out_weight
    )
    swap = [(0, 1), (1, 0)]
    mixer_part = summed(keep, send, "c", swap)
    mixer_part = summed(*halves(mixer_part, side == 0), "q", swap)
    mixer_part = summed(*halves(mixer_part, column < 2), "p", [(i, i ^ 2) for i in range(groups)])
    mixer_part = summed(*halves(mixer_part, column % 2 == 0), "p", [(i, i ^ 1) for i in range(groups)])

    results = expert_ffn(slot_rows, (pack, pack_c, pack_q, pack_qc), sharers * hidden_part)
    back = results.reshape(experts, share, parts, piece).transpose(0, 2, 1, 3)
    back = lax.all_to_all(
        back.reshape(experts * parts, share, piece), ALL, split_axis=0, concat_axis=0, tiled=True
    )
    pieces = combined(table, back.reshape(experts, groups, capacity, piece), mixer_part, pick_count)

    mine = lax.all_gather(pieces, ("p", "q"), axis=0, tiled=False)
    other = flipped(mine, "c")
    return assembled(core, mine, other, length)


def solution(mesh):
    experts, parts = mesh.devices.shape
    finer = Mesh(mesh.devices.reshape(experts, parts // 4, 2, 2), ALL)
    return jax.shard_map(
        on_device,
        mesh=finer,
        in_specs=(
            P("ep", None),
            P(),
            P(None, TP),
            P(None, TP),
            P(None, TP),
            P(None, TP),
            P(TP, None),
            P("ep", None),
            P(),
            P("ep", None),
            P("ep", None),
            P("ep", None, TP),
            P("ep", None, TP),
            P("ep", TP, None),
        ),
        out_specs=(P("ep", None), P("ep", None)),
        check_vma=False,
    )
```

```python
import functools

import jax
import jax.numpy as jnp
from jax import lax
from jax.experimental import pallas as pl
from jax.experimental.pallas import tpu as pltpu
from jax.sharding import Mesh, PartitionSpec as P

TP = ("p", "q", "c")
ALL = ("ep", "p", "q", "c")
VM = pl.BlockSpec(memory_space=pltpu.VMEM)
HBM = pl.BlockSpec(memory_space=pltpu.HBM)


def flipped(value, axis):
    return lax.ppermute(value, axis, [(0, 1), (1, 0)])


def route_kernel(
    quarter_ref,
    ids_ref,
    weights_ref,
    rows_ref,
    gain_ref,
    out_ref,
    picks_ref,
    *,
    experts,
    capacity,
    share,
):
    picks, tokens = ids_ref.shape
    slots = out_ref.shape[0]
    expert = lax.broadcasted_iota(jnp.int32, (experts, tokens), 0)
    named = [ids_ref[k : k + 1, :] == expert for k in range(picks)]
    both = functools.reduce(jnp.logical_or, named)
    row = lax.broadcasted_iota(jnp.int32, (tokens, tokens), 0)
    col = lax.broadcasted_iota(jnp.int32, (tokens, tokens), 1)
    earlier = jnp.dot(
        jnp.where(both, 1.0, 0.0).astype(jnp.bfloat16),
        jnp.where(row < col, 1.0, 0.0).astype(jnp.bfloat16),
        preferred_element_type=jnp.float32,
    )
    slot = lax.broadcasted_iota(jnp.int32, (slots, tokens), 0)
    slot_key = slot // share * capacity + slot % share + quarter_ref[0] * share
    chosen, lines = None, []
    for k in range(picks):
        rank = jnp.sum(jnp.where(named[k], earlier, 0.0), axis=0, keepdims=True).astype(jnp.int32)
        key = ids_ref[k : k + 1, :] * capacity + rank
        lines.append(key.astype(jnp.float32))
        here = slot_key == key
        chosen = here if chosen is None else jnp.logical_or(chosen, here)
    lines += [weights_ref[k : k + 1, :] for k in range(picks)]
    line = lax.broadcasted_iota(jnp.int32, (128, tokens), 0)
    table = jnp.zeros((128, tokens), jnp.float32)
    for i, value in enumerate(lines):
        table = jnp.where(line == i, value, table)
    picks_ref[...] = table.T
    values = rows_ref[...].astype(jnp.float32)
    scaled = values * lax.rsqrt(jnp.mean(values * values, axis=-1, keepdims=True) + 1e-06)
    normed = (scaled * gain_ref[...]).astype(jnp.bfloat16)
    out_ref[...] = jnp.dot(
        jnp.where(chosen, 1.0, 0.0).astype(jnp.bfloat16), normed, preferred_element_type=jnp.float32
    ).astype(jnp.bfloat16)


def routed_slots(quarter, ids, weights, rows, gain, experts, capacity, share):
    tokens, width = rows.shape
    return pl.pallas_call(
        functools.partial(route_kernel, experts=experts, capacity=capacity, share=share),
        out_shape=(
            jax.ShapeDtypeStruct((experts * share, width), jnp.bfloat16),
            jax.ShapeDtypeStruct((tokens, 128), jnp.float32),
        ),
        in_specs=[pl.BlockSpec(memory_space=pltpu.SMEM), VM, VM, VM, VM],
        out_specs=(VM, VM),
        name="route",
    )(quarter.reshape(1), ids.T, weights.T, rows, gain.reshape(1, -1))


def mixer_kernel(
    core_ref, before_ref, rows_ref, gain_ref, inner_ref, gate_in_ref, gate_out_ref, taps_ref, out_w_ref, keep_ref, send_ref, ext_ref
):
    def normed(ref):
        values = ref[...].astype(jnp.float32)
        scaled = values * lax.rsqrt(jnp.mean(values * values, axis=-1, keepdims=True) + 1e-06)
        return (scaled * gain_ref[...]).astype(jnp.bfloat16)

    def projected(x, ref):
        return lax.dot_general(x, ref[...], (((1,), (1,)), ((), ())), preferred_element_type=jnp.float32)

    def conv_input(x):
        return (projected(x, gate_in_ref) * projected(x, inner_ref)).astype(jnp.bfloat16).astype(jnp.float32)

    lead, length = before_ref.shape[0], rows_ref.shape[0]
    x = normed(rows_ref)
    ext_ref[:lead, :] = conv_input(normed(before_ref))
    ext_ref[lead:, :] = conv_input(x)
    taps = taps_ref.shape[0]
    conv_out = None
    for j in range(taps):
        at = lead - (taps - 1) + j
        term = taps_ref[j : j + 1, :] * ext_ref[at : at + length, :]
        conv_out = term if conv_out is None else conv_out + term
    gated = (projected(x, gate_out_ref) * conv_out).astype(jnp.bfloat16)
    middle = out_w_ref.shape[1] // 2
    left = jnp.dot(gated, out_w_ref[:, :middle], preferred_element_type=jnp.float32).astype(jnp.bfloat16)
    right = jnp.dot(gated, out_w_ref[:, middle:], preferred_element_type=jnp.float32).astype(jnp.bfloat16)
    first = core_ref[0] == 0
    keep_ref[...] = jnp.where(first, left, right)
    send_ref[...] = jnp.where(first, right, left)


def mixer_terms(core, before, rows, gain, inner, gate_in, gate_out, taps, out_weight):
    length, width = rows.shape
    half = jax.ShapeDtypeStruct((length, width // 2), jnp.bfloat16)
    return pl.pallas_call(
        mixer_kernel,
        out_shape=(half, half),
        in_specs=[pl.BlockSpec(memory_space=pltpu.SMEM)] + [VM] * 8,
        out_specs=(VM, VM),
        scratch_shapes=[pltpu.VMEM((before.shape[0] + length, taps.shape[1]), jnp.float32)],
        name="mixer",
    )(core.reshape(1), before, rows, gain.reshape(1, -1), inner.T, gate_in.T, gate_out.T, taps, out_weight)


def summed(kept, sent, axis, pairs):
    received = lax.ppermute(sent, axis, pairs)
    return (kept.astype(jnp.float32) + received.astype(jnp.float32)).astype(jnp.bfloat16)


def halves(value, first):
    middle = value.shape[1] // 2
    left, right = value[:, :middle], value[:, middle:]
    return jnp.where(first, left, right), jnp.where(first, right, left)


def ffn_kernel(x_hbm, a0, a1, a2, a3, b0, b1, b2, b3, out_ref, x_ref, gu_ref, down_ref, hid_ref, sems):
    width = x_ref.shape[1]
    part = a0.shape[1]
    lead = b0.shape[0] - part
    x_copy = pltpu.make_async_copy(x_hbm, x_ref, sems.at[0])
    x_copy.start()
    copies = []
    for i, (a, b) in enumerate(((a0, b0), (a1, b1), (a2, b2), (a3, b3))):
        gate = pltpu.make_async_copy(
            a.at[pl.ds(0, width), :], gu_ref.at[i, :, pl.ds(0, part)], sems.at[3 * i + 1]
        )
        up = pltpu.make_async_copy(
            a.at[pl.ds(width, width), :], gu_ref.at[i, :, pl.ds(part, part)], sems.at[3 * i + 2]
        )
        down = pltpu.make_async_copy(
            b.at[pl.ds(lead, part), :], down_ref.at[pl.ds(i * part, part), :], sems.at[3 * i + 3]
        )
        gate.start()
        up.start()
        copies.append((gate, up, down))
    for _, _, down in copies:
        down.start()
    x_copy.wait()
    for i, (gate, up, _) in enumerate(copies):
        gate.wait()
        up.wait()
        acts = jnp.dot(x_ref[...], gu_ref[i], preferred_element_type=jnp.float32)
        g = acts[:, :part]
        hid_ref[:, i * part : (i + 1) * part] = (g / (1.0 + jnp.exp(-g)) * acts[:, part:]).astype(jnp.bfloat16)
    for _, _, down in copies:
        down.wait()
    cols = 512
    for n in range(0, width, cols):
        out_ref[:, n : n + cols] = jnp.dot(
            hid_ref[...], down_ref[:, n : n + cols], preferred_element_type=jnp.float32
        ).astype(jnp.bfloat16)


def expert_ffn(x, packs, hidden):
    rows, width = x.shape
    part = packs[0].shape[1]
    views = [wide_view(w, width) for w in packs]
    return pl.pallas_call(
        ffn_kernel,
        out_shape=jax.ShapeDtypeStruct(x.shape, jnp.bfloat16),
        in_specs=[HBM] * 9,
        out_specs=VM,
        scratch_shapes=[
            pltpu.VMEM((rows, width), jnp.bfloat16),
            pltpu.VMEM((4, width, 2 * part), jnp.bfloat16),
            pltpu.VMEM((hidden, width), jnp.bfloat16),
            pltpu.VMEM((rows, hidden), jnp.bfloat16),
            pltpu.SemaphoreType.DMA((13,)),
        ],
        cost_estimate=pl.CostEstimate(
            flops=6 * rows * width * hidden, bytes_accessed=8 * 2**20, transcendentals=rows * hidden
        ),
        name="expert_ffn",
    )(x, *packs, *views)


def narrow_view(value, part):
    rows, width = value.shape
    return value.reshape(rows // 8, 8, width // part, part).transpose(0, 2, 1, 3).reshape(-1, part)


def wide_view(value, width):
    _, part = value.shape
    return value.reshape(-1, width // part, 8, part).transpose(0, 2, 1, 3).reshape(-1, width)


def combine_kernel(picks_ref, rows_hbm, main_ref, tail_ref, rows_ref, sem, *, picks):
    copy = pltpu.make_async_copy(rows_hbm, rows_ref, sem)
    copy.start()
    experts, groups, capacity, width = rows_ref.shape
    tokens = picks_ref.shape[0]
    slots = experts * capacity
    column = lax.broadcasted_iota(jnp.int32, (tokens, slots), 1)
    spread = jnp.zeros((tokens, slots), jnp.float32)
    for k in range(picks):
        key = picks_ref[:, k : k + 1].astype(jnp.int32)
        spread = jnp.where(column == key, picks_ref[:, picks + k : picks + k + 1], spread)
    high = spread.astype(jnp.bfloat16)
    low = (spread - high.astype(jnp.float32)).astype(jnp.bfloat16)
    copy.wait()
    total = jnp.zeros((tokens, 2 * width), jnp.float32)
    for g in range(0, groups, 2):
        rows = jnp.concatenate(
            [rows_ref[:, g].reshape(slots, width), rows_ref[:, g + 1].reshape(slots, width)], axis=1
        )
        total = total + jnp.dot(high, rows, preferred_element_type=jnp.float32)
        total = total + jnp.dot(low, rows, preferred_element_type=jnp.float32)
    result = (total[:, :width] + total[:, width:]).astype(jnp.bfloat16)
    head = main_ref.shape[0]
    main_ref[...] = result[:head]
    for i in range(tail_ref.shape[0]):
        tail_ref[i] = result[head:]


def combined(table, rows, picks, copies, tail):
    tokens, width = table.shape[0], rows.shape[-1]
    return pl.pallas_call(
        functools.partial(combine_kernel, picks=picks),
        out_shape=(
            jax.ShapeDtypeStruct((tokens - tail, width), jnp.bfloat16),
            jax.ShapeDtypeStruct((copies, tail, width), jnp.bfloat16),
        ),
        in_specs=[VM, HBM],
        out_specs=(VM, VM),
        scratch_shapes=[pltpu.VMEM(rows.shape, jnp.bfloat16), pltpu.SemaphoreType.DMA],
        name="combine",
    )(table, rows)


def column_kernel(*refs, places):
    *parts, out_ref, sems = refs
    copies, at = [], 0
    for part in parts:
        count, rows, width = part.shape
        for i in range(count):
            copies.append(
                pltpu.make_async_copy(
                    part.at[i],
                    out_ref.at[pl.ds(at, rows), pl.ds(places[i] * width, width)],
                    sems.at[len(copies)],
                )
            )
            copies[-1].start()
        at += rows
    for copy in copies:
        copy.wait()


def side_by_side(places, *parts):
    count, _, width = parts[0].shape
    return pl.pallas_call(
        functools.partial(column_kernel, places=places),
        out_shape=jax.ShapeDtypeStruct((sum(p.shape[1] for p in parts), count * width), jnp.bfloat16),
        in_specs=[HBM] * len(parts),
        out_specs=VM,
        scratch_shapes=[pltpu.SemaphoreType.DMA((count * len(parts),))],
        name="side_by_side",
    )(*parts)


def on_device(
    mixer_rows,
    mixer_gain,
    inner_weight,
    gate_in_weight,
    gate_out_weight,
    conv_taps,
    mixer_out_weight,
    routed_rows,
    routed_gain,
    route_ids,
    route_weights,
    expert_gate,
    expert_up,
    expert_down,
):
    experts = lax.axis_size("ep")
    groups = lax.axis_size("p")
    parts = lax.axis_size(TP)
    sharers = lax.axis_size(("q", "c"))
    quarter = lax.axis_index(("q", "c"))
    tok_count, pick_count = route_ids.shape
    width = routed_rows.shape[1]
    capacity = 2 * tok_count * pick_count // experts
    share = capacity // sharers
    piece = width // parts
    hidden_part = expert_gate.shape[2]

    core, side = lax.axis_index("c"), lax.axis_index("q")
    column = lax.axis_index("p")
    length = mixer_rows.shape[0]

    pack = jnp.concatenate([expert_gate[0], expert_up[0], narrow_view(expert_down[0], hidden_part)], axis=0)
    pack_q = flipped(pack, "q")

    lead = 8
    before = lax.ppermute(mixer_rows[length - lead :], "ep", [(i, i + 1) for i in range(experts - 1)])

    outgoing, table = routed_slots(
        quarter, route_ids, route_weights, routed_rows, routed_gain, experts, capacity, share
    )
    slot_rows = lax.all_to_all(
        outgoing.reshape(experts, share, width), "ep", split_axis=0, concat_axis=0, tiled=True
    ).reshape(experts * share, width)
    pack_c = flipped(pack, "c")
    pack_qc = flipped(pack_q, "c")

    keep, send = mixer_terms(
        core, before, mixer_rows, mixer_gain, inner_weight, gate_in_weight, gate_out_weight, conv_taps, mixer_out_weight
    )
    swap = [(0, 1), (1, 0)]
    mixer_part = summed(keep, send, "c", swap)
    mixer_part = summed(*halves(mixer_part, side == 0), "q", swap)
    mixer_part = summed(*halves(mixer_part, column < 2), "p", [(i, i ^ 2) for i in range(groups)])
    mixer_part = summed(*halves(mixer_part, column % 2 == 0), "p", [(i, i ^ 1) for i in range(groups)])

    results = expert_ffn(slot_rows, (pack, pack_c, pack_q, pack_qc), sharers * hidden_part)
    back = results.reshape(experts, share, parts, piece).transpose(0, 2, 1, 3)
    back = lax.all_to_all(
        back.reshape(experts * parts, share, piece), ALL, split_axis=0, concat_axis=0, tiled=True
    )
    mixer_all = lax.all_gather(mixer_part, TP, axis=0, tiled=False)
    mixer_whole = side_by_side([i % 2 * 8 + i // 2 % 2 * 4 + i // 4 for i in range(parts)], mixer_all)

    main, tail = combined(table, back.reshape(experts, groups, capacity, piece), pick_count, parts, 8)
    tail_all = lax.all_to_all(tail, TP, split_axis=0, concat_axis=0, tiled=True)
    main_all = lax.all_gather(main, TP, axis=0, tiled=False)
    return mixer_whole, side_by_side(list(range(parts)), main_all, tail_all)


def solution(mesh):
    experts, parts = mesh.devices.shape
    finer = Mesh(mesh.devices.reshape(experts, parts // 4, 2, 2), ALL)
    return jax.shard_map(
        on_device,
        mesh=finer,
        in_specs=(
            P("ep", None),
            P(),
            P(None, TP),
            P(None, TP),
            P(None, TP),
            P(None, TP),
            P(TP, None),
            P("ep", None),
            P(),
            P("ep", None),
            P("ep", None),
            P("ep", None, TP),
            P("ep", None, TP),
            P("ep", TP, None),
        ),
        out_specs=(P("ep", None), P("ep", None)),
        check_vma=False,
    )
```

```python
import functools

import jax
import jax.numpy as jnp
from jax import lax
from jax.experimental import pallas as pl
from jax.experimental.pallas import tpu as pltpu
from jax.sharding import Mesh, PartitionSpec as P

TP = ("p", "q", "c")
ALL = ("ep", "p", "q", "c")
VM = pl.BlockSpec(memory_space=pltpu.VMEM)
HBM = pl.BlockSpec(memory_space=pltpu.HBM)


def flipped(value, axis):
    return lax.ppermute(value, axis, [(0, 1), (1, 0)])


def route_kernel(
    quarter_ref,
    ids_ref,
    weights_ref,
    rows_ref,
    gain_ref,
    out_ref,
    picks_ref,
    *,
    experts,
    capacity,
    share,
):
    picks, tokens = ids_ref.shape
    slots = out_ref.shape[0]
    expert = lax.broadcasted_iota(jnp.int32, (experts, tokens), 0)
    named = [ids_ref[k : k + 1, :] == expert for k in range(picks)]
    both = functools.reduce(jnp.logical_or, named)
    row = lax.broadcasted_iota(jnp.int32, (tokens, tokens), 0)
    col = lax.broadcasted_iota(jnp.int32, (tokens, tokens), 1)
    earlier = jnp.dot(
        jnp.where(both, 1.0, 0.0).astype(jnp.bfloat16),
        jnp.where(row < col, 1.0, 0.0).astype(jnp.bfloat16),
        preferred_element_type=jnp.float32,
    )
    slot = lax.broadcasted_iota(jnp.int32, (slots, tokens), 0)
    slot_key = slot // share * capacity + slot % share + quarter_ref[0] * share
    chosen, lines = None, []
    for k in range(picks):
        rank = jnp.sum(jnp.where(named[k], earlier, 0.0), axis=0, keepdims=True).astype(jnp.int32)
        key = ids_ref[k : k + 1, :] * capacity + rank
        lines.append(key.astype(jnp.float32))
        here = slot_key == key
        chosen = here if chosen is None else jnp.logical_or(chosen, here)
    lines += [weights_ref[k : k + 1, :] for k in range(picks)]
    line = lax.broadcasted_iota(jnp.int32, (128, tokens), 0)
    table = jnp.zeros((128, tokens), jnp.float32)
    for i, value in enumerate(lines):
        table = jnp.where(line == i, value, table)
    picks_ref[...] = table.T
    values = rows_ref[...].astype(jnp.float32)
    scaled = values * lax.rsqrt(jnp.mean(values * values, axis=-1, keepdims=True) + 1e-06)
    normed = (scaled * gain_ref[...]).astype(jnp.bfloat16)
    out_ref[...] = jnp.dot(
        jnp.where(chosen, 1.0, 0.0).astype(jnp.bfloat16), normed, preferred_element_type=jnp.float32
    ).astype(jnp.bfloat16)


def routed_slots(quarter, ids, weights, rows, gain, experts, capacity, share):
    tokens, width = rows.shape
    return pl.pallas_call(
        functools.partial(route_kernel, experts=experts, capacity=capacity, share=share),
        out_shape=(
            jax.ShapeDtypeStruct((experts * share, width), jnp.bfloat16),
            jax.ShapeDtypeStruct((tokens, 128), jnp.float32),
        ),
        in_specs=[pl.BlockSpec(memory_space=pltpu.SMEM), VM, VM, VM, VM],
        out_specs=(VM, VM),
        name="route",
    )(quarter.reshape(1), ids.T, weights.T, rows, gain.reshape(1, -1))


def mixer_kernel(
    core_ref, before_ref, rows_ref, gain_ref, inner_ref, gate_in_ref, gate_out_ref, taps_ref, out_w_ref, keep_ref, send_ref, ext_ref
):
    def normed(ref):
        values = ref[...].astype(jnp.float32)
        scaled = values * lax.rsqrt(jnp.mean(values * values, axis=-1, keepdims=True) + 1e-06)
        return (scaled * gain_ref[...]).astype(jnp.bfloat16)

    def projected(x, ref):
        return lax.dot_general(x, ref[...], (((1,), (1,)), ((), ())), preferred_element_type=jnp.float32)

    def conv_input(x):
        return (projected(x, gate_in_ref) * projected(x, inner_ref)).astype(jnp.bfloat16).astype(jnp.float32)

    lead, length = before_ref.shape[0], rows_ref.shape[0]
    x = normed(rows_ref)
    ext_ref[:lead, :] = conv_input(normed(before_ref))
    ext_ref[lead:, :] = conv_input(x)
    taps = taps_ref.shape[0]
    conv_out = None
    for j in range(taps):
        at = lead - (taps - 1) + j
        term = taps_ref[j : j + 1, :] * ext_ref[at : at + length, :]
        conv_out = term if conv_out is None else conv_out + term
    gated = (projected(x, gate_out_ref) * conv_out).astype(jnp.bfloat16)
    middle = out_w_ref.shape[1] // 2
    left = jnp.dot(gated, out_w_ref[:, :middle], preferred_element_type=jnp.float32).astype(jnp.bfloat16)
    right = jnp.dot(gated, out_w_ref[:, middle:], preferred_element_type=jnp.float32).astype(jnp.bfloat16)
    first = core_ref[0] == 0
    piece = keep_ref.shape[2]
    for i in range(keep_ref.shape[0]):
        a, b = left[:, i * piece : (i + 1) * piece], right[:, i * piece : (i + 1) * piece]
        keep_ref[i] = jnp.where(first, a, b)
        send_ref[i] = jnp.where(first, b, a)


def mixer_terms(core, before, rows, gain, inner, gate_in, gate_out, taps, out_weight, blocks):
    length, width = rows.shape
    half = jax.ShapeDtypeStruct((blocks, length, width // (2 * blocks)), jnp.bfloat16)
    return pl.pallas_call(
        mixer_kernel,
        out_shape=(half, half),
        in_specs=[pl.BlockSpec(memory_space=pltpu.SMEM)] + [VM] * 8,
        out_specs=(VM, VM),
        scratch_shapes=[pltpu.VMEM((before.shape[0] + length, taps.shape[1]), jnp.float32)],
        name="mixer",
    )(core.reshape(1), before, rows, gain.reshape(1, -1), inner.T, gate_in.T, gate_out.T, taps, out_weight)


def summed(kept, sent, axis, pairs):
    received = lax.ppermute(sent, axis, pairs)
    return (kept.astype(jnp.float32) + received.astype(jnp.float32)).astype(jnp.bfloat16)


def halves(value, first):
    middle = value.shape[0] // 2
    left, right = value[:middle], value[middle:]
    return jnp.where(first, left, right), jnp.where(first, right, left)


def spread_kernel(me_ref, kept_ref, received_ref, *out_refs):
    count = kept_ref.shape[0]
    for step, out_ref in enumerate(out_refs):
        block = lax.rem(me_ref[0] + step, count)
        total = kept_ref[block].astype(jnp.float32) + received_ref[block].astype(jnp.float32)
        out_ref[...] = total.astype(jnp.bfloat16)


def spread_blocks(me, kept, received):
    count = kept.shape[0]
    return pl.pallas_call(
        spread_kernel,
        out_shape=tuple(jax.ShapeDtypeStruct(kept.shape[1:], jnp.bfloat16) for _ in range(count)),
        in_specs=[pl.BlockSpec(memory_space=pltpu.SMEM), VM, VM],
        out_specs=(VM,) * count,
        name="spread_blocks",
    )(me.reshape(1), kept, received)


def ffn_kernel(x_hbm, a0, a1, a2, a3, b0, b1, b2, b3, out_ref, x_ref, gu_ref, down_ref, hid_ref, sems):
    width = x_ref.shape[1]
    part = a0.shape[1]
    lead = b0.shape[0] - part
    x_copy = pltpu.make_async_copy(x_hbm, x_ref, sems.at[0])
    x_copy.start()
    copies = []
    for i, (a, b) in enumerate(((a0, b0), (a1, b1), (a2, b2), (a3, b3))):
        gate = pltpu.make_async_copy(
            a.at[pl.ds(0, width), :], gu_ref.at[i, :, pl.ds(0, part)], sems.at[3 * i + 1]
        )
        up = pltpu.make_async_copy(
            a.at[pl.ds(width, width), :], gu_ref.at[i, :, pl.ds(part, part)], sems.at[3 * i + 2]
        )
        down = pltpu.make_async_copy(
            b.at[pl.ds(lead, part), :], down_ref.at[pl.ds(i * part, part), :], sems.at[3 * i + 3]
        )
        gate.start()
        up.start()
        copies.append((gate, up, down))
    for _, _, down in copies:
        down.start()
    x_copy.wait()
    for i, (gate, up, _) in enumerate(copies):
        gate.wait()
        up.wait()
        acts = jnp.dot(x_ref[...], gu_ref[i], preferred_element_type=jnp.float32)
        g = acts[:, :part]
        hid_ref[:, i * part : (i + 1) * part] = (g / (1.0 + jnp.exp(-g)) * acts[:, part:]).astype(jnp.bfloat16)
    for _, _, down in copies:
        down.wait()
    cols = 512
    for n in range(0, width, cols):
        out_ref[:, n : n + cols] = jnp.dot(
            hid_ref[...], down_ref[:, n : n + cols], preferred_element_type=jnp.float32
        ).astype(jnp.bfloat16)


def expert_ffn(x, packs, hidden):
    rows, width = x.shape
    part = packs[0].shape[1]
    views = [wide_view(w, width) for w in packs]
    return pl.pallas_call(
        ffn_kernel,
        out_shape=jax.ShapeDtypeStruct(x.shape, jnp.bfloat16),
        in_specs=[HBM] * 9,
        out_specs=VM,
        scratch_shapes=[
            pltpu.VMEM((rows, width), jnp.bfloat16),
            pltpu.VMEM((4, width, 2 * part), jnp.bfloat16),
            pltpu.VMEM((hidden, width), jnp.bfloat16),
            pltpu.VMEM((rows, hidden), jnp.bfloat16),
            pltpu.SemaphoreType.DMA((13,)),
        ],
        cost_estimate=pl.CostEstimate(
            flops=6 * rows * width * hidden, bytes_accessed=8 * 2**20, transcendentals=rows * hidden
        ),
        name="expert_ffn",
    )(x, *packs, *views)


def narrow_view(value, part):
    rows, width = value.shape
    return value.reshape(rows // 8, 8, width // part, part).transpose(0, 2, 1, 3).reshape(-1, part)


def wide_view(value, width):
    _, part = value.shape
    return value.reshape(-1, width // part, 8, part).transpose(0, 2, 1, 3).reshape(-1, width)


def combine_kernel(picks_ref, rows_ref, mixer_ref, out_ref, *, picks):
    experts, groups, capacity, width = rows_ref.shape
    tokens = picks_ref.shape[0]
    slots = experts * capacity
    column = lax.broadcasted_iota(jnp.int32, (tokens, slots), 1)
    spread = jnp.zeros((tokens, slots), jnp.float32)
    for k in range(picks):
        key = picks_ref[:, k : k + 1].astype(jnp.int32)
        spread = jnp.where(column == key, picks_ref[:, picks + k : picks + k + 1], spread)
    high = spread.astype(jnp.bfloat16)
    low = (spread - high.astype(jnp.float32)).astype(jnp.bfloat16)
    total = jnp.zeros((tokens, 2 * width), jnp.float32)
    for g in range(0, groups, 2):
        rows = jnp.concatenate(
            [rows_ref[:, g].reshape(slots, width), rows_ref[:, g + 1].reshape(slots, width)], axis=1
        )
        total = total + jnp.dot(high, rows, preferred_element_type=jnp.float32)
        total = total + jnp.dot(low, rows, preferred_element_type=jnp.float32)
    length = mixer_ref.shape[0]
    out_ref[:length, :] = mixer_ref[...]
    out_ref[length:, :] = (total[:, :width] + total[:, width:]).astype(jnp.bfloat16)


def combined(table, rows, mixer_part, picks):
    return pl.pallas_call(
        functools.partial(combine_kernel, picks=picks),
        out_shape=jax.ShapeDtypeStruct((mixer_part.shape[0] + table.shape[0], rows.shape[-1]), jnp.bfloat16),
        in_specs=[VM] * 3,
        out_specs=VM,
        name="combine",
    )(table, rows, mixer_part)


def place_kernel(core_ref, parts_ref, *refs, length, flip):
    mixer_ref, routed_ref, sems = refs[-3:]
    count, rows, piece = parts_ref.shape
    core = 1 - core_ref[0] if flip else core_ref[0]
    copies = []
    for i in range(count):
        at = pl.multiple_of((2 * i + core) * piece, piece)
        copies.append((length, rows - length, routed_ref, at))
        at = pl.multiple_of((core * count + i % 2 * (count // 2) + i // 2) * piece, piece)
        copies.append((0, length, mixer_ref, at))
    copies = [
        pltpu.make_async_copy(
            parts_ref.at[n // 2, pl.ds(start, size), :], target.at[:, pl.ds(at, piece)], sems.at[n]
        )
        for n, (start, size, target, at) in enumerate(copies)
    ]
    for copy in copies:
        copy.start()
    for copy in copies:
        copy.wait()


def placed(core, parts, length, wholes=()):
    count, rows, piece = parts.shape
    return pl.pallas_call(
        functools.partial(place_kernel, length=length, flip=bool(wholes)),
        out_shape=(
            jax.ShapeDtypeStruct((length, 2 * count * piece), jnp.bfloat16),
            jax.ShapeDtypeStruct((rows - length, 2 * count * piece), jnp.bfloat16),
        ),
        in_specs=[pl.BlockSpec(memory_space=pltpu.SMEM), VM] + [HBM] * len(wholes),
        out_specs=(HBM, HBM),
        input_output_aliases={2: 0, 3: 1} if wholes else {},
        scratch_shapes=[pltpu.SemaphoreType.DMA((2 * count,))],
        name="placed",
    )(core.reshape(1), parts, *wholes)


def on_device(
    mixer_rows,
    mixer_gain,
    inner_weight,
    gate_in_weight,
    gate_out_weight,
    conv_taps,
    mixer_out_weight,
    routed_rows,
    routed_gain,
    route_ids,
    route_weights,
    expert_gate,
    expert_up,
    expert_down,
):
    experts = lax.axis_size("ep")
    groups = lax.axis_size("p")
    parts = lax.axis_size(TP)
    sharers = lax.axis_size(("q", "c"))
    quarter = lax.axis_index(("q", "c"))
    tok_count, pick_count = route_ids.shape
    width = routed_rows.shape[1]
    capacity = 2 * tok_count * pick_count // experts
    share = capacity // sharers
    piece = width // parts
    hidden_part = expert_gate.shape[2]

    core, side = lax.axis_index("c"), lax.axis_index("q")
    column = lax.axis_index("p")
    length = mixer_rows.shape[0]

    pack = jnp.concatenate([expert_gate[0], expert_up[0], narrow_view(expert_down[0], hidden_part)], axis=0)
    pack_q = flipped(pack, "q")

    lead = 8
    before = lax.ppermute(mixer_rows[length - lead :], "ep", [(i, i + 1) for i in range(experts - 1)])

    outgoing, table = routed_slots(
        quarter, route_ids, route_weights, routed_rows, routed_gain, experts, capacity, share
    )
    slot_rows = lax.all_to_all(
        outgoing.reshape(experts, share, width), "ep", split_axis=0, concat_axis=0, tiled=True
    ).reshape(experts * share, width)
    pack_c = flipped(pack, "c")
    pack_qc = flipped(pack_q, "c")

    keep, send = mixer_terms(
        core, before, mixer_rows, mixer_gain, inner_weight, gate_in_weight, gate_out_weight, conv_taps, mixer_out_weight, parts // 2
    )
    swap = [(0, 1), (1, 0)]
    mixer_part = summed(keep, send, "c", swap)
    kept, sent = halves(mixer_part, side == 0)
    received = lax.ppermute(sent, "q", swap)
    blocks = spread_blocks(column, kept, received)
    total = blocks[0].astype(jnp.float32)
    for step in range(1, groups):
        block = lax.ppermute(blocks[step], "p", [(i, (i + step) % groups) for i in range(groups)])
        total = total + block.astype(jnp.float32)
    mixer_part = total.astype(jnp.bfloat16)

    results = expert_ffn(slot_rows, (pack, pack_c, pack_q, pack_qc), sharers * hidden_part)
    back = results.reshape(experts, share, parts, piece).transpose(0, 2, 1, 3)
    back = lax.all_to_all(
        back.reshape(experts * parts, share, piece), ALL, split_axis=0, concat_axis=0, tiled=True
    )
    pieces = combined(table, back.reshape(experts, groups, capacity, piece), mixer_part, pick_count)

    mine = lax.all_gather(pieces, ("p", "q"), axis=0, tiled=False)
    other = flipped(mine, "c")
    wholes = placed(core, mine, length)
    return placed(core, other, length, wholes)


def solution(mesh):
    experts, parts = mesh.devices.shape
    finer = Mesh(mesh.devices.reshape(experts, parts // 4, 2, 2), ALL)
    return jax.shard_map(
        on_device,
        mesh=finer,
        in_specs=(
            P("ep", None),
            P(),
            P(None, TP),
            P(None, TP),
            P(None, TP),
            P(None, TP),
            P(TP, None),
            P("ep", None),
            P(),
            P("ep", None),
            P("ep", None),
            P("ep", None, TP),
            P("ep", None, TP),
            P("ep", TP, None),
        ),
        out_specs=(P("ep", None), P("ep", None)),
        check_vma=False,
    )
```

```python
import functools

import jax
import jax.numpy as jnp
from jax import lax
from jax.experimental import pallas as pl
from jax.experimental.pallas import tpu as pltpu
from jax.sharding import Mesh, PartitionSpec as P

TP = ("p", "q", "c")
ALL = ("ep", "p", "q", "c")
VM = pl.BlockSpec(memory_space=pltpu.VMEM)
HBM = pl.BlockSpec(memory_space=pltpu.HBM)


def flipped(value, axis):
    return lax.ppermute(value, axis, [(0, 1), (1, 0)])


def route_kernel(
    quarter_ref,
    ids_ref,
    weights_ref,
    rows_ref,
    gain_ref,
    last_ref,
    out_ref,
    picks_ref,
    halo_ref,
    *,
    experts,
    capacity,
    share,
):
    halo_ref[...] = last_ref[...]
    picks, tokens = ids_ref.shape
    slots = out_ref.shape[0]
    expert = lax.broadcasted_iota(jnp.int32, (experts, tokens), 0)
    named = [ids_ref[k : k + 1, :] == expert for k in range(picks)]
    both = functools.reduce(jnp.logical_or, named)
    row = lax.broadcasted_iota(jnp.int32, (tokens, tokens), 0)
    col = lax.broadcasted_iota(jnp.int32, (tokens, tokens), 1)
    earlier = jnp.dot(
        jnp.where(both, 1.0, 0.0).astype(jnp.bfloat16),
        jnp.where(row < col, 1.0, 0.0).astype(jnp.bfloat16),
        preferred_element_type=jnp.float32,
    )
    slot = lax.broadcasted_iota(jnp.int32, (slots, tokens), 0)
    slot_key = slot // share * capacity + slot % share + quarter_ref[0] * share
    chosen, lines = None, []
    for k in range(picks):
        rank = jnp.sum(jnp.where(named[k], earlier, 0.0), axis=0, keepdims=True).astype(jnp.int32)
        key = ids_ref[k : k + 1, :] * capacity + rank
        lines.append(key.astype(jnp.float32))
        here = slot_key == key
        chosen = here if chosen is None else jnp.logical_or(chosen, here)
    lines += [weights_ref[k : k + 1, :] for k in range(picks)]
    line = lax.broadcasted_iota(jnp.int32, (128, tokens), 0)
    table = jnp.zeros((128, tokens), jnp.float32)
    for i, value in enumerate(lines):
        table = jnp.where(line == i, value, table)
    picks_ref[...] = table.T
    values = rows_ref[...].astype(jnp.float32)
    scaled = values * lax.rsqrt(jnp.mean(values * values, axis=-1, keepdims=True) + 1e-06)
    normed = (scaled * gain_ref[...]).astype(jnp.bfloat16)
    out_ref[...] = jnp.dot(
        jnp.where(chosen, 1.0, 0.0).astype(jnp.bfloat16), normed, preferred_element_type=jnp.float32
    ).astype(jnp.bfloat16)


def routed_slots(quarter, ids, weights, rows, gain, mixer_rows, lead, experts, capacity, share):
    tokens, width = rows.shape
    return pl.pallas_call(
        functools.partial(route_kernel, experts=experts, capacity=capacity, share=share),
        out_shape=(
            jax.ShapeDtypeStruct((experts * share, width), jnp.bfloat16),
            jax.ShapeDtypeStruct((tokens, 128), jnp.float32),
            jax.ShapeDtypeStruct((lead, width), jnp.bfloat16),
        ),
        grid=(1,),
        in_specs=[
            pl.BlockSpec(memory_space=pltpu.SMEM),
            VM,
            VM,
            VM,
            VM,
            pl.BlockSpec((lead, width), lambda i: (mixer_rows.shape[0] // lead - 1, 0)),
        ],
        out_specs=(VM, VM, VM),
        name="route",
    )(quarter.reshape(1), ids.T, weights.T, rows, gain.reshape(1, -1), mixer_rows)


def mixer_kernel(
    core_ref, before_ref, rows_ref, gain_ref, inner_ref, gate_in_ref, gate_out_ref, taps_ref, out_w_ref, keep_ref, send_ref, ext_ref
):
    def normed(ref):
        values = ref[...].astype(jnp.float32)
        scaled = values * lax.rsqrt(jnp.mean(values * values, axis=-1, keepdims=True) + 1e-06)
        return (scaled * gain_ref[...]).astype(jnp.bfloat16)

    def projected(x, ref):
        return lax.dot_general(x, ref[...], (((1,), (1,)), ((), ())), preferred_element_type=jnp.float32)

    def conv_input(x):
        return (projected(x, gate_in_ref) * projected(x, inner_ref)).astype(jnp.bfloat16).astype(jnp.float32)

    lead, length = before_ref.shape[0], rows_ref.shape[0]
    x = normed(rows_ref)
    ext_ref[:lead, :] = conv_input(normed(before_ref))
    ext_ref[lead:, :] = conv_input(x)
    taps = taps_ref.shape[0]
    conv_out = None
    for j in range(taps):
        at = lead - (taps - 1) + j
        term = taps_ref[j : j + 1, :] * ext_ref[at : at + length, :]
        conv_out = term if conv_out is None else conv_out + term
    gated = (projected(x, gate_out_ref) * conv_out).astype(jnp.bfloat16)
    middle = out_w_ref.shape[1] // 2
    left = jnp.dot(gated, out_w_ref[:, :middle], preferred_element_type=jnp.float32).astype(jnp.bfloat16)
    right = jnp.dot(gated, out_w_ref[:, middle:], preferred_element_type=jnp.float32).astype(jnp.bfloat16)
    first = core_ref[0] == 0
    piece = keep_ref.shape[2]
    for i in range(keep_ref.shape[0]):
        a, b = left[:, i * piece : (i + 1) * piece], right[:, i * piece : (i + 1) * piece]
        keep_ref[i] = jnp.where(first, a, b)
        send_ref[i] = jnp.where(first, b, a)


def mixer_terms(core, before, rows, gain, inner, gate_in, gate_out, taps, out_weight, blocks):
    length, width = rows.shape
    half = jax.ShapeDtypeStruct((blocks, length, width // (2 * blocks)), jnp.bfloat16)
    return pl.pallas_call(
        mixer_kernel,
        out_shape=(half, half),
        in_specs=[pl.BlockSpec(memory_space=pltpu.SMEM)] + [VM] * 8,
        out_specs=(VM, VM),
        scratch_shapes=[pltpu.VMEM((before.shape[0] + length, taps.shape[1]), jnp.float32)],
        name="mixer",
    )(core.reshape(1), before, rows, gain.reshape(1, -1), inner.T, gate_in.T, gate_out.T, taps, out_weight)


def summed(kept, sent, axis, pairs):
    received = lax.ppermute(sent, axis, pairs)
    return (kept.astype(jnp.float32) + received.astype(jnp.float32)).astype(jnp.bfloat16)


def halves(value, first):
    middle = value.shape[0] // 2
    left, right = value[:middle], value[middle:]
    return jnp.where(first, left, right), jnp.where(first, right, left)


def spread_kernel(me_ref, kept_ref, received_ref, *out_refs):
    count = kept_ref.shape[0]
    for step, out_ref in enumerate(out_refs):
        block = lax.rem(me_ref[0] + step, count)
        total = kept_ref[block].astype(jnp.float32) + received_ref[block].astype(jnp.float32)
        out_ref[...] = total.astype(jnp.bfloat16)


def spread_blocks(me, kept, received):
    count = kept.shape[0]
    return pl.pallas_call(
        spread_kernel,
        out_shape=tuple(jax.ShapeDtypeStruct(kept.shape[1:], jnp.bfloat16) for _ in range(count)),
        in_specs=[pl.BlockSpec(memory_space=pltpu.SMEM), VM, VM],
        out_specs=(VM,) * count,
        name="spread_blocks",
    )(me.reshape(1), kept, received)


def ffn_kernel(x_hbm, a0, a1, a2, a3, b0, b1, b2, b3, out_ref, x_ref, gu_ref, down_ref, hid_ref, sems):
    width = x_ref.shape[1]
    part = a0.shape[1]
    lead = b0.shape[0] - part
    x_copy = pltpu.make_async_copy(x_hbm, x_ref, sems.at[0])
    x_copy.start()
    weights, downs = [], []
    for i, (a, b) in enumerate(((a0, b0), (a1, b1), (a2, b2), (a3, b3))):
        gate = pltpu.make_async_copy(
            a.at[pl.ds(0, width), :], gu_ref.at[i, :, pl.ds(0, part)], sems.at[3 * i + 1]
        )
        up = pltpu.make_async_copy(
            a.at[pl.ds(width, width), :], gu_ref.at[i, :, pl.ds(part, part)], sems.at[3 * i + 2]
        )
        down = pltpu.make_async_copy(
            b.at[pl.ds(lead, part), :], down_ref.at[pl.ds(i * part, part), :], sems.at[3 * i + 3]
        )
        weights.append((gate, up))
        downs.append(down)
    later = weights[2:] + [downs]
    for copy in weights[0] + weights[1]:
        copy.start()
    x_copy.wait()
    for i, slices in enumerate(weights):
        for copy in slices:
            copy.wait()
        if i < len(later):
            for copy in later[i]:
                copy.start()
        acts = jnp.dot(x_ref[...], gu_ref[i], preferred_element_type=jnp.float32)
        g = acts[:, :part]
        hid_ref[:, i * part : (i + 1) * part] = (g / (1.0 + jnp.exp(-g)) * acts[:, part:]).astype(jnp.bfloat16)
    for down in downs:
        down.wait()
    cols = 512
    for n in range(0, width, cols):
        out_ref[:, n : n + cols] = jnp.dot(
            hid_ref[...], down_ref[:, n : n + cols], preferred_element_type=jnp.float32
        ).astype(jnp.bfloat16)


def expert_ffn(x, packs, hidden):
    rows, width = x.shape
    part = packs[0].shape[1]
    views = [wide_view(w, width) for w in packs]
    return pl.pallas_call(
        ffn_kernel,
        out_shape=jax.ShapeDtypeStruct(x.shape, jnp.bfloat16),
        in_specs=[HBM] * 9,
        out_specs=VM,
        scratch_shapes=[
            pltpu.VMEM((rows, width), jnp.bfloat16),
            pltpu.VMEM((4, width, 2 * part), jnp.bfloat16),
            pltpu.VMEM((hidden, width), jnp.bfloat16),
            pltpu.VMEM((rows, hidden), jnp.bfloat16),
            pltpu.SemaphoreType.DMA((13,)),
        ],
        cost_estimate=pl.CostEstimate(
            flops=6 * rows * width * hidden, bytes_accessed=8 * 2**20, transcendentals=rows * hidden
        ),
        name="expert_ffn",
    )(x, *packs, *views)


def narrow_view(value, part):
    rows, width = value.shape
    return value.reshape(rows // 8, 8, width // part, part).transpose(0, 2, 1, 3).reshape(-1, part)


def wide_view(value, width):
    _, part = value.shape
    return value.reshape(-1, width // part, 8, part).transpose(0, 2, 1, 3).reshape(-1, width)


def combine_kernel(core_ref, picks_ref, rows_ref, keep_ref, send_ref, *, picks, share, capacity):
    experts, groups, pair, width = rows_ref.shape
    tokens = picks_ref.shape[0]
    slots = experts * pair
    core = core_ref[0]
    slot = lax.broadcasted_iota(jnp.int32, (tokens, slots), 1)
    column = slot // pair * capacity + slot % pair // share * (2 * share) + slot % share + core * share
    spread = jnp.zeros((tokens, slots), jnp.float32)
    for k in range(picks):
        key = picks_ref[:, k : k + 1].astype(jnp.int32)
        spread = jnp.where(column == key, picks_ref[:, picks + k : picks + k + 1], spread)
    high = spread.astype(jnp.bfloat16)
    low = (spread - high.astype(jnp.float32)).astype(jnp.bfloat16)
    total = jnp.zeros((tokens, width), jnp.float32)
    for g in range(groups):
        rows = rows_ref[:, g].reshape(slots, width)
        total = total + jnp.dot(high, rows, preferred_element_type=jnp.float32)
        total = total + jnp.dot(low, rows, preferred_element_type=jnp.float32)
    left, right = total[:, : width // 2], total[:, width // 2 :]
    keep_ref[...] = jnp.where(core == 0, left, right)
    send_ref[...] = jnp.where(core == 0, right, left).astype(jnp.bfloat16)


def combined(core, table, rows, picks, share, capacity):
    half = (table.shape[0], rows.shape[-1] // 2)
    return pl.pallas_call(
        functools.partial(combine_kernel, picks=picks, share=share, capacity=capacity),
        out_shape=(jax.ShapeDtypeStruct(half, jnp.float32), jax.ShapeDtypeStruct(half, jnp.bfloat16)),
        in_specs=[pl.BlockSpec(memory_space=pltpu.SMEM), VM, VM],
        out_specs=(VM, VM),
        name="combine",
    )(core.reshape(1), table, rows)


def place_kernel(core_ref, parts_ref, *refs, length, flip):
    mixer_ref, routed_ref, sems = refs[-3:]
    count, rows, piece = parts_ref.shape
    core = 1 - core_ref[0] if flip else core_ref[0]
    copies = []
    for i in range(count):
        at = pl.multiple_of((2 * i + core) * piece, piece)
        copies.append((length, rows - length, routed_ref, at))
        at = pl.multiple_of((core * count + i % 2 * (count // 2) + i // 2) * piece, piece)
        copies.append((0, length, mixer_ref, at))
    copies = [
        pltpu.make_async_copy(
            parts_ref.at[n // 2, pl.ds(start, size), :], target.at[:, pl.ds(at, piece)], sems.at[n]
        )
        for n, (start, size, target, at) in enumerate(copies)
    ]
    for copy in copies:
        copy.start()
    for copy in copies:
        copy.wait()


def placed(core, parts, length, wholes=()):
    count, rows, piece = parts.shape
    return pl.pallas_call(
        functools.partial(place_kernel, length=length, flip=bool(wholes)),
        out_shape=(
            jax.ShapeDtypeStruct((length, 2 * count * piece), jnp.bfloat16),
            jax.ShapeDtypeStruct((rows - length, 2 * count * piece), jnp.bfloat16),
        ),
        in_specs=[pl.BlockSpec(memory_space=pltpu.SMEM), VM] + [HBM] * len(wholes),
        out_specs=(HBM, HBM),
        input_output_aliases={2: 0, 3: 1} if wholes else {},
        scratch_shapes=[pltpu.SemaphoreType.DMA((2 * count,))],
        name="placed",
    )(core.reshape(1), parts, *wholes)


def on_device(
    mixer_rows,
    mixer_gain,
    inner_weight,
    gate_in_weight,
    gate_out_weight,
    conv_taps,
    mixer_out_weight,
    routed_rows,
    routed_gain,
    route_ids,
    route_weights,
    expert_gate,
    expert_up,
    expert_down,
):
    experts = lax.axis_size("ep")
    groups = lax.axis_size("p")
    parts = lax.axis_size(TP)
    sharers = lax.axis_size(("q", "c"))
    quarter = lax.axis_index(("q", "c"))
    tok_count, pick_count = route_ids.shape
    width = routed_rows.shape[1]
    capacity = 2 * tok_count * pick_count // experts
    share = capacity // sharers
    piece = width // parts
    hidden_part = expert_gate.shape[2]

    core, side = lax.axis_index("c"), lax.axis_index("q")
    column = lax.axis_index("p")
    length = mixer_rows.shape[0]

    pack = jnp.concatenate([expert_gate[0], expert_up[0], narrow_view(expert_down[0], hidden_part)], axis=0)
    pack_q = flipped(pack, "q")

    outgoing, table, last_rows = routed_slots(
        quarter, route_ids, route_weights, routed_rows, routed_gain, mixer_rows, 8, experts, capacity, share
    )
    before = lax.ppermute(last_rows, "ep", [(i, i + 1) for i in range(experts - 1)])
    slot_rows = lax.all_to_all(
        outgoing.reshape(experts, share, width), "ep", split_axis=0, concat_axis=0, tiled=True
    ).reshape(experts * share, width)
    pack_c = flipped(pack, "c")
    pack_qc = flipped(pack_q, "c")

    keep, send = mixer_terms(
        core, before, mixer_rows, mixer_gain, inner_weight, gate_in_weight, gate_out_weight, conv_taps, mixer_out_weight, parts // 2
    )
    swap = [(0, 1), (1, 0)]
    mixer_part = summed(keep, send, "c", swap)
    kept, sent = halves(mixer_part, side == 0)
    received = lax.ppermute(sent, "q", swap)
    blocks = spread_blocks(column, kept, received)
    total = blocks[0].astype(jnp.float32)
    for step in range(1, groups):
        block = lax.ppermute(blocks[step], "p", [(i, (i + step) % groups) for i in range(groups)])
        total = total + block.astype(jnp.float32)
    mixer_part = total.astype(jnp.bfloat16)

    results = expert_ffn(slot_rows, (pack, pack_c, pack_q, pack_qc), sharers * hidden_part)
    chips = parts // 2
    back = results.reshape(experts, share, chips, 2 * piece).transpose(0, 2, 1, 3)
    back = lax.all_to_all(
        back.reshape(experts * chips, share, 2 * piece), ALL[:3], split_axis=0, concat_axis=0, tiled=True
    )
    kept, sent = combined(
        core, table, back.reshape(experts, groups, 2 * share, 2 * piece), pick_count, share, capacity
    )
    received = flipped(sent, "c")
    routed_part = (kept + received.astype(jnp.float32)).astype(jnp.bfloat16)

    pieces = jnp.concatenate([mixer_part, routed_part], axis=0)
    mine = lax.all_gather(pieces, ("p", "q"), axis=0, tiled=False)
    other = flipped(mine, "c")
    wholes = placed(core, mine, length)
    return placed(core, other, length, wholes)


def solution(mesh):
    experts, parts = mesh.devices.shape
    finer = Mesh(mesh.devices.reshape(experts, parts // 4, 2, 2), ALL)
    return jax.shard_map(
        on_device,
        mesh=finer,
        in_specs=(
            P("ep", None),
            P(),
            P(None, TP),
            P(None, TP),
            P(None, TP),
            P(None, TP),
            P(TP, None),
            P("ep", None),
            P(),
            P("ep", None),
            P("ep", None),
            P("ep", None, TP),
            P("ep", None, TP),
            P("ep", TP, None),
        ),
        out_specs=(P("ep", None), P("ep", None)),
        check_vma=False,
    )
```

```python
import functools

import jax
import jax.numpy as jnp
from jax import lax
from jax.experimental import pallas as pl
from jax.experimental.pallas import tpu as pltpu
from jax.sharding import Mesh, PartitionSpec as P

TP = ("p", "q", "c")
ALL = ("ep", "p", "q", "c")
VM = pl.BlockSpec(memory_space=pltpu.VMEM)
HBM = pl.BlockSpec(memory_space=pltpu.HBM)


def flipped(value, axis):
    return lax.ppermute(value, axis, [(0, 1), (1, 0)])


def route_kernel(
    quarter_ref,
    ids_ref,
    weights_ref,
    rows_ref,
    gain_ref,
    last_ref,
    out_ref,
    picks_ref,
    halo_ref,
    *,
    experts,
    capacity,
    share,
):
    halo_ref[...] = last_ref[...]
    picks, tokens = ids_ref.shape
    slots = out_ref.shape[0]
    expert = lax.broadcasted_iota(jnp.int32, (experts, tokens), 0)
    named = [ids_ref[k : k + 1, :] == expert for k in range(picks)]
    both = functools.reduce(jnp.logical_or, named)
    row = lax.broadcasted_iota(jnp.int32, (tokens, tokens), 0)
    col = lax.broadcasted_iota(jnp.int32, (tokens, tokens), 1)
    earlier = jnp.dot(
        jnp.where(both, 1.0, 0.0).astype(jnp.bfloat16),
        jnp.where(row < col, 1.0, 0.0).astype(jnp.bfloat16),
        preferred_element_type=jnp.float32,
    )
    slot = lax.broadcasted_iota(jnp.int32, (slots, tokens), 0)
    slot_key = slot // share * capacity + slot % share + quarter_ref[0] * share
    chosen, lines = None, []
    for k in range(picks):
        rank = jnp.sum(jnp.where(named[k], earlier, 0.0), axis=0, keepdims=True).astype(jnp.int32)
        key = ids_ref[k : k + 1, :] * capacity + rank
        lines.append(key.astype(jnp.float32))
        here = slot_key == key
        chosen = here if chosen is None else jnp.logical_or(chosen, here)
    lines += [weights_ref[k : k + 1, :] for k in range(picks)]
    line = lax.broadcasted_iota(jnp.int32, (128, tokens), 0)
    table = jnp.zeros((128, tokens), jnp.float32)
    for i, value in enumerate(lines):
        table = jnp.where(line == i, value, table)
    picks_ref[...] = table.T
    values = rows_ref[...].astype(jnp.float32)
    scaled = values * lax.rsqrt(jnp.mean(values * values, axis=-1, keepdims=True) + 1e-06)
    normed = (scaled * gain_ref[...]).astype(jnp.bfloat16)
    out_ref[...] = jnp.dot(
        jnp.where(chosen, 1.0, 0.0).astype(jnp.bfloat16), normed, preferred_element_type=jnp.float32
    ).astype(jnp.bfloat16)


def routed_slots(quarter, ids, weights, rows, gain, mixer_rows, lead, experts, capacity, share):
    tokens, width = rows.shape
    return pl.pallas_call(
        functools.partial(route_kernel, experts=experts, capacity=capacity, share=share),
        out_shape=(
            jax.ShapeDtypeStruct((experts * share, width), jnp.bfloat16),
            jax.ShapeDtypeStruct((tokens, 128), jnp.float32),
            jax.ShapeDtypeStruct((lead, width), jnp.bfloat16),
        ),
        grid=(1,),
        in_specs=[
            pl.BlockSpec(memory_space=pltpu.SMEM),
            VM,
            VM,
            VM,
            VM,
            pl.BlockSpec((lead, width), lambda i: (mixer_rows.shape[0] // lead - 1, 0)),
        ],
        out_specs=(VM, VM, VM),
        name="route",
    )(quarter.reshape(1), ids.T, weights.T, rows, gain.reshape(1, -1), mixer_rows)


def mixer_kernel(
    core_ref, before_ref, rows_ref, gain_ref, inner_ref, gate_in_ref, gate_out_ref, taps_ref, out_w_ref, keep_ref, send_ref, ext_ref
):
    def normed(ref):
        values = ref[...].astype(jnp.float32)
        scaled = values * lax.rsqrt(jnp.mean(values * values, axis=-1, keepdims=True) + 1e-06)
        return (scaled * gain_ref[...]).astype(jnp.bfloat16)

    def projected(x, ref):
        return lax.dot_general(x, ref[...], (((1,), (1,)), ((), ())), preferred_element_type=jnp.float32)

    def conv_input(x):
        return (projected(x, gate_in_ref) * projected(x, inner_ref)).astype(jnp.bfloat16).astype(jnp.float32)

    lead, length = before_ref.shape[0], rows_ref.shape[0]
    x = normed(rows_ref)
    ext_ref[:lead, :] = conv_input(normed(before_ref))
    ext_ref[lead:, :] = conv_input(x)
    taps = taps_ref.shape[0]
    conv_out = None
    for j in range(taps):
        at = lead - (taps - 1) + j
        term = taps_ref[j : j + 1, :] * ext_ref[at : at + length, :]
        conv_out = term if conv_out is None else conv_out + term
    gated = (projected(x, gate_out_ref) * conv_out).astype(jnp.bfloat16)
    middle = out_w_ref.shape[1] // 2
    left = jnp.dot(gated, out_w_ref[:, :middle], preferred_element_type=jnp.float32).astype(jnp.bfloat16)
    right = jnp.dot(gated, out_w_ref[:, middle:], preferred_element_type=jnp.float32).astype(jnp.bfloat16)
    first = core_ref[0] == 0
    piece = keep_ref.shape[2]
    for i in range(keep_ref.shape[0]):
        a, b = left[:, i * piece : (i + 1) * piece], right[:, i * piece : (i + 1) * piece]
        keep_ref[i] = jnp.where(first, a, b)
        send_ref[i] = jnp.where(first, b, a)


def mixer_terms(core, before, rows, gain, inner, gate_in, gate_out, taps, out_weight, blocks):
    length, width = rows.shape
    half = jax.ShapeDtypeStruct((blocks, length, width // (2 * blocks)), jnp.bfloat16)
    return pl.pallas_call(
        mixer_kernel,
        out_shape=(half, half),
        in_specs=[pl.BlockSpec(memory_space=pltpu.SMEM)] + [VM] * 8,
        out_specs=(VM, VM),
        scratch_shapes=[pltpu.VMEM((before.shape[0] + length, taps.shape[1]), jnp.float32)],
        name="mixer",
    )(core.reshape(1), before, rows, gain.reshape(1, -1), inner.T, gate_in.T, gate_out.T, taps, out_weight)


def summed(kept, sent, axis, pairs):
    received = lax.ppermute(sent, axis, pairs)
    return (kept.astype(jnp.float32) + received.astype(jnp.float32)).astype(jnp.bfloat16)


def halves(value, first):
    middle = value.shape[0] // 2
    left, right = value[:middle], value[middle:]
    return jnp.where(first, left, right), jnp.where(first, right, left)


def spread_kernel(me_ref, kept_ref, received_ref, *out_refs):
    count = kept_ref.shape[0]
    for step, out_ref in enumerate(out_refs):
        block = lax.rem(me_ref[0] + step, count)
        total = kept_ref[block].astype(jnp.float32) + received_ref[block].astype(jnp.float32)
        out_ref[...] = total.astype(jnp.bfloat16)


def spread_blocks(me, kept, received):
    count = kept.shape[0]
    return pl.pallas_call(
        spread_kernel,
        out_shape=tuple(jax.ShapeDtypeStruct(kept.shape[1:], jnp.bfloat16) for _ in range(count)),
        in_specs=[pl.BlockSpec(memory_space=pltpu.SMEM), VM, VM],
        out_specs=(VM,) * count,
        name="spread_blocks",
    )(me.reshape(1), kept, received)


def ffn_kernel(x_hbm, a0, a1, a2, a3, b0, b1, b2, b3, out_ref, x_ref, gu_ref, down_ref, hid_ref, sems):
    width = x_ref.shape[1]
    part = a0.shape[1]
    lead = b0.shape[0] - part
    x_copy = pltpu.make_async_copy(x_hbm, x_ref, sems.at[0])
    x_copy.start()
    copies = []
    for i, (a, b) in enumerate(((a0, b0), (a1, b1), (a2, b2), (a3, b3))):
        gate = pltpu.make_async_copy(
            a.at[pl.ds(0, width), :], gu_ref.at[i, :, pl.ds(0, part)], sems.at[3 * i + 1]
        )
        up = pltpu.make_async_copy(
            a.at[pl.ds(width, width), :], gu_ref.at[i, :, pl.ds(part, part)], sems.at[3 * i + 2]
        )
        down = pltpu.make_async_copy(
            b.at[pl.ds(lead, part), :], down_ref.at[pl.ds(i * part, part), :], sems.at[3 * i + 3]
        )
        gate.start()
        up.start()
        copies.append((gate, up, down))
    for _, _, down in copies:
        down.start()
    x_copy.wait()
    for i, (gate, up, _) in enumerate(copies):
        gate.wait()
        up.wait()
        acts = jnp.dot(x_ref[...], gu_ref[i], preferred_element_type=jnp.float32)
        g = acts[:, :part]
        hid_ref[:, i * part : (i + 1) * part] = (g / (1.0 + jnp.exp(-g)) * acts[:, part:]).astype(jnp.bfloat16)
    for _, _, down in copies:
        down.wait()
    cols = 512
    for n in range(0, width, cols):
        out_ref[:, n : n + cols] = jnp.dot(
            hid_ref[...], down_ref[:, n : n + cols], preferred_element_type=jnp.float32
        ).astype(jnp.bfloat16)


def expert_ffn(x, packs, hidden):
    rows, width = x.shape
    part = packs[0].shape[1]
    views = [wide_view(w, width) for w in packs]
    return pl.pallas_call(
        ffn_kernel,
        out_shape=jax.ShapeDtypeStruct(x.shape, jnp.bfloat16),
        in_specs=[HBM] * 9,
        out_specs=VM,
        scratch_shapes=[
            pltpu.VMEM((rows, width), jnp.bfloat16),
            pltpu.VMEM((4, width, 2 * part), jnp.bfloat16),
            pltpu.VMEM((hidden, width), jnp.bfloat16),
            pltpu.VMEM((rows, hidden), jnp.bfloat16),
            pltpu.SemaphoreType.DMA((13,)),
        ],
        cost_estimate=pl.CostEstimate(
            flops=6 * rows * width * hidden, bytes_accessed=8 * 2**20, transcendentals=rows * hidden
        ),
        name="expert_ffn",
    )(x, *packs, *views)


def narrow_view(value, part):
    rows, width = value.shape
    return value.reshape(rows // 8, 8, width // part, part).transpose(0, 2, 1, 3).reshape(-1, part)


def wide_view(value, width):
    _, part = value.shape
    return value.reshape(-1, width // part, 8, part).transpose(0, 2, 1, 3).reshape(-1, width)


def combine_kernel(picks_ref, rows_ref, mixer_ref, out_ref, *, picks):
    experts, groups, capacity, width = rows_ref.shape
    tokens = picks_ref.shape[0]
    slots = experts * capacity
    column = lax.broadcasted_iota(jnp.int32, (tokens, slots), 1)
    spread = jnp.zeros((tokens, slots), jnp.float32)
    for k in range(picks):
        key = picks_ref[:, k : k + 1].astype(jnp.int32)
        spread = jnp.where(column == key, picks_ref[:, picks + k : picks + k + 1], spread)
    high = spread.astype(jnp.bfloat16)
    low = (spread - high.astype(jnp.float32)).astype(jnp.bfloat16)
    total = jnp.zeros((tokens, 2 * width), jnp.float32)
    for g in range(0, groups, 2):
        rows = jnp.concatenate(
            [rows_ref[:, g].reshape(slots, width), rows_ref[:, g + 1].reshape(slots, width)], axis=1
        )
        total = total + jnp.dot(high, rows, preferred_element_type=jnp.float32)
        total = total + jnp.dot(low, rows, preferred_element_type=jnp.float32)
    length = mixer_ref.shape[0]
    out_ref[:length, :] = mixer_ref[...]
    out_ref[length:, :] = (total[:, :width] + total[:, width:]).astype(jnp.bfloat16)


def combined(table, rows, mixer_part, picks):
    return pl.pallas_call(
        functools.partial(combine_kernel, picks=picks),
        out_shape=jax.ShapeDtypeStruct((mixer_part.shape[0] + table.shape[0], rows.shape[-1]), jnp.bfloat16),
        in_specs=[VM] * 3,
        out_specs=VM,
        name="combine",
    )(table, rows, mixer_part)


def place_kernel(core_ref, parts_ref, *refs, length, flip):
    mixer_ref, routed_ref, sems = refs[-3:]
    count, rows, piece = parts_ref.shape
    core = 1 - core_ref[0] if flip else core_ref[0]
    copies = []
    for i in range(count):
        at = pl.multiple_of((2 * i + core) * piece, piece)
        copies.append((length, rows - length, routed_ref, at))
        at = pl.multiple_of((core * count + i % 2 * (count // 2) + i // 2) * piece, piece)
        copies.append((0, length, mixer_ref, at))
    copies = [
        pltpu.make_async_copy(
            parts_ref.at[n // 2, pl.ds(start, size), :], target.at[:, pl.ds(at, piece)], sems.at[n]
        )
        for n, (start, size, target, at) in enumerate(copies)
    ]
    for copy in copies:
        copy.start()
    for copy in copies:
        copy.wait()


def placed(core, parts, length, wholes=()):
    count, rows, piece = parts.shape
    return pl.pallas_call(
        functools.partial(place_kernel, length=length, flip=bool(wholes)),
        out_shape=(
            jax.ShapeDtypeStruct((length, 2 * count * piece), jnp.bfloat16),
            jax.ShapeDtypeStruct((rows - length, 2 * count * piece), jnp.bfloat16),
        ),
        in_specs=[pl.BlockSpec(memory_space=pltpu.SMEM), VM] + [HBM] * len(wholes),
        out_specs=(HBM, HBM),
        input_output_aliases={2: 0, 3: 1} if wholes else {},
        scratch_shapes=[pltpu.SemaphoreType.DMA((2 * count,))],
        name="placed",
    )(core.reshape(1), parts, *wholes)


def on_device(
    mixer_rows,
    mixer_gain,
    inner_weight,
    gate_in_weight,
    gate_out_weight,
    conv_taps,
    mixer_out_weight,
    routed_rows,
    routed_gain,
    route_ids,
    route_weights,
    expert_gate,
    expert_up,
    expert_down,
):
    experts = lax.axis_size("ep")
    groups = lax.axis_size("p")
    parts = lax.axis_size(TP)
    sharers = lax.axis_size(("q", "c"))
    quarter = lax.axis_index(("q", "c"))
    tok_count, pick_count = route_ids.shape
    width = routed_rows.shape[1]
    capacity = 2 * tok_count * pick_count // experts
    share = capacity // sharers
    piece = width // parts
    hidden_part = expert_gate.shape[2]

    core, side = lax.axis_index("c"), lax.axis_index("q")
    column = lax.axis_index("p")
    length = mixer_rows.shape[0]

    pack = jnp.concatenate([expert_gate[0], expert_up[0], narrow_view(expert_down[0], hidden_part)], axis=0)
    pack_q = flipped(pack, "q")

    outgoing, table, last_rows = routed_slots(
        quarter, route_ids, route_weights, routed_rows, routed_gain, mixer_rows, 8, experts, capacity, share
    )
    before = lax.ppermute(last_rows, "ep", [(i, i + 1) for i in range(experts - 1)])
    slot_rows = lax.all_to_all(
        outgoing.reshape(experts, share, width), "ep", split_axis=0, concat_axis=0, tiled=True
    ).reshape(experts * share, width)
    pack_c = flipped(pack, "c")
    pack_qc = flipped(pack_q, "c")

    keep, send = mixer_terms(
        core, before, mixer_rows, mixer_gain, inner_weight, gate_in_weight, gate_out_weight, conv_taps, mixer_out_weight, parts // 2
    )
    swap = [(0, 1), (1, 0)]
    mixer_part = summed(keep, send, "c", swap)
    kept, sent = halves(mixer_part, side == 0)
    received = lax.ppermute(sent, "q", swap)
    blocks = spread_blocks(column, kept, received)
    total = blocks[0].astype(jnp.float32)
    for step in range(1, groups):
        block = lax.ppermute(blocks[step], "p", [(i, (i + step) % groups) for i in range(groups)])
        total = total + block.astype(jnp.float32)
    mixer_part = total.astype(jnp.bfloat16)

    results = expert_ffn(slot_rows, (pack, pack_c, pack_q, pack_qc), sharers * hidden_part)
    back = results.reshape(experts, share, parts, piece).transpose(0, 2, 1, 3)
    back = lax.all_to_all(
        back.reshape(experts * parts, share, piece), ALL, split_axis=0, concat_axis=0, tiled=True
    )
    pieces = combined(table, back.reshape(experts, groups, capacity, piece), mixer_part, pick_count)

    mine = lax.all_gather(pieces, ("p", "q"), axis=0, tiled=False)
    other = flipped(mine, "c")
    wholes = placed(core, mine, length)
    return placed(core, other, length, wholes)


def solution(mesh):
    experts, parts = mesh.devices.shape
    finer = Mesh(mesh.devices.reshape(experts, parts // 4, 2, 2), ALL)
    return jax.shard_map(
        on_device,
        mesh=finer,
        in_specs=(
            P("ep", None),
            P(),
            P(None, TP),
            P(None, TP),
            P(None, TP),
            P(None, TP),
            P(TP, None),
            P("ep", None),
            P(),
            P("ep", None),
            P("ep", None),
            P("ep", None, TP),
            P("ep", None, TP),
            P("ep", TP, None),
        ),
        out_specs=(P("ep", None), P("ep", None)),
        check_vma=False,
    )
```
